512 devices in a mesh: kv: 64 (over z, y), tp: 8 (over x, core).
Axes of the slice: x: 4, y: 8, z: 8, core: 2. Of those that a mesh axis runs over, the one named last changes fastest.
Arguments:
- tokens: bfloat16 [512, 2048], P(None, ('kv', 'tp')), may hold values from -16 to 16
- mix_gain: float32 [2048], P('kv'), may hold values from 0.1 to 1.9
- query_weight: bfloat16 [2048, 2048], P('kv', 'tp'), may hold values from -0.125 to 0.125
- key_weight: bfloat16 [2048, 2048], P('kv', 'tp'), may hold values from -0.125 to 0.125
- value_weight: bfloat16 [2048, 2048], P('kv', 'tp'), may hold values from -0.125 to 0.125
- beta_weight: bfloat16 [2048, 16], P('kv', 'tp'), may hold values from -0.125 to 0.125
- decay_weight: bfloat16 [2048, 16], P('kv', 'tp'), may hold values from -0.125 to 0.125
- decay_rate: float32 [16], P('tp'), may hold values from 0.05 to 1
- prior_state: float32 [512, 16, 128, 128], P('kv', 'tp'), may hold values from -1.5 to 1.5
- tail_keys: bfloat16 [512, 16, 64, 128], P('kv', 'tp'), may hold values from -6 to 6
- tail_values: bfloat16 [512, 16, 64, 128], P('kv', 'tp'), may hold values from -6 to 6
- tail_beta: float32 [512, 16, 64], P('kv', 'tp'), may hold values from 0.1 to 0.9
- tail_decay: float32 [512, 16, 64], P('kv', 'tp'), may hold values from -2 to 0
- lengths: int32 [512], P('kv'), may hold values from 1 to 64, 13107 in all
- out_weight: bfloat16 [2048, 2048], P('tp', 'kv'), may hold values from -0.375 to 0.375
- mlp_gain: float32 [2048], P('kv'), may hold values from 0.1 to 1.9
- up_weight: bfloat16 [2048, 8192], P('kv', 'tp'), may hold values from -0.125 to 0.125
- down_weight: bfloat16 [8192, 2048], P('tp', 'kv'), may hold values from -0.0625 to 0.0625
Outputs:
- mixed: bfloat16 [512, 2048], P(None, ('kv', 'tp'))
The draws below stay inside these ranges and needn't reach their ends.
All inputs are finite; a program needn't handle non-finite values. No bound on the sum of `lengths` on one device may be relied on, other than what follows from the above.
Results may differ from the reference program's by a relative error of at most 0.013.
Values may be sent and summed in bfloat16 or wider, within the bound.
A program may use at most 64 MiB of HBM per device.

```python
import math
import jax
import jax.numpy as jnp
import numpy as np
from jax import lax

D = 2048
HEAD_COUNT = 16
HEAD_DIM = 128
FF = 8192
PENDING_KEYS = 64
INNER = 2048
SEQUENCE_BATCH = 512


def draw_tokens(key, part):
    first = jax.random.fold_in(key, 11)
    second = jax.random.fold_in(key, 12)
    base = jax.random.normal(first, (SEQUENCE_BATCH, D), jnp.float32)
    column = jnp.arange(D, dtype=jnp.float32) / D
    rising = jnp.exp(math.log(6.0) * (column - 0.5)) * jax.random.uniform(second, (D,), jnp.float32, 0.6, 1.4)
    value_vectors = base * rising[None, :]
    return jnp.clip(value_vectors, -16.0, 16.0).astype(jnp.bfloat16)


def draw_tail_decay(key, part):
    pick_key = jax.random.fold_in(key, 21)
    slow_key = jax.random.fold_in(key, 22)
    quick_key = jax.random.fold_in(key, 23)
    factor_key = jax.random.fold_in(key, 24)
    rough_key = jax.random.fold_in(key, 25)
    spike_random_key = jax.random.fold_in(key, 26)
    drop_key = jax.random.fold_in(key, 27)
    quick = jax.random.randint(pick_key, (HEAD_COUNT,), 0, 2) == 1
    slow_rate = jnp.exp(jax.random.uniform(slow_key, (HEAD_COUNT,), jnp.float32, math.log(0.001), math.log(0.005)))
    quick_rate = jnp.exp(jax.random.uniform(quick_key, (HEAD_COUNT,), jnp.float32, math.log(0.04), math.log(0.1)))
    per_head_rate = jnp.where(quick, quick_rate, slow_rate)
    sequence_multiplier = jnp.exp(jax.random.uniform(factor_key, (SEQUENCE_BATCH, 1, 1), jnp.float32, math.log(0.5), math.log(2.0)))
    jitter_amount = jax.random.uniform(rough_key, (SEQUENCE_BATCH, HEAD_COUNT, PENDING_KEYS), jnp.float32, 0.5, 1.5)
    spike_sample = jax.random.randint(spike_random_key, (SEQUENCE_BATCH, HEAD_COUNT, PENDING_KEYS), 0, 32) == 0
    discard_fraction = jnp.log(jax.random.uniform(drop_key, (SEQUENCE_BATCH, HEAD_COUNT, PENDING_KEYS), jnp.float32, 0.5, 0.8))
    value_vectors = -per_head_rate[None, :, None] * sequence_multiplier * jitter_amount + jnp.where(spike_sample, discard_fraction, 0.0)
    return jnp.clip(value_vectors, -2.0, 0.0)


def levels(rng, extent, pieces, smallest, top_value):
    loudness = 1.0
    for axis_at, parts in pieces:
        draws = jax.random.uniform(jax.random.fold_in(jax.random.fold_in(rng, 6), axis_at), (parts,), jnp.float32, smallest / len(pieces), top_value / len(pieces))
        loudness = loudness * jnp.repeat(jnp.exp(draws), extent[axis_at] // parts).reshape((-1,) + (1,) * (len(extent) - 1 - axis_at))
    return loudness


def length_profile(count, total, reach, slope):
    weights = [(1 << 20) // math.isqrt(grade ** slope) + 1 for grade in range(2, count + 1)]
    rest, given = total - reach - (count - 1), [1] * (count - 1)
    while rest > 0:
        movable = [i for i in range(count - 1) if given[i] < reach]
        pool, remaining = sum([weights[i] for i in movable]), rest
        for i in movable:
            more = min(reach - given[i], max(1, remaining * weights[i] // pool), rest)
            given[i] = given[i] + more
            rest = rest - more
    return np.array([reach] + given)


def ragged(stream_key, count, total, reach, skew):
    if count == 2:
        one = jax.random.randint(stream_key, (), max(1, total - reach), min(reach, total - 1) + 1)
        return jnp.stack([one, total - one])
    sizes = jnp.asarray(length_profile(count, total, reach, skew), jnp.int32)
    couples = (count - 1) // 2
    source_of, receiver = sizes[1:1 + 2 * couples:2], sizes[2:2 + 2 * couples:2]
    room = jnp.minimum(source_of - 1, reach - receiver)
    passed = jax.random.randint(jax.random.fold_in(stream_key, 1), (couples,), 0, 1 << 20) % (room + 1)
    sizes = sizes.at[1:1 + 2 * couples:2].set(source_of - passed).at[2:2 + 2 * couples:2].set(receiver + passed)
    return sizes[jax.random.permutation(jax.random.fold_in(stream_key, 2), count)]


def gaussian(rng, dims, deviation, limit, cuts=(), held_as=jnp.bfloat16):
    drawn = deviation * jax.random.normal(rng, dims, jnp.float32)
    if cuts:
        drawn = drawn * levels(rng, dims, cuts, -0.22, 0.18)
    return jnp.clip(drawn, -limit, limit).astype(held_as)


def setup_inputs(seed: int = 0) -> dict:
    key_list = jax.random.split(jax.random.key(seed), 19)
    tokens = draw_tokens(jax.random.fold_in(key_list[18], 71), 0)
    mix_gain = jnp.clip(1.0 + 0.18 * jax.random.normal(key_list[1], (D,), jnp.float32), 0.1, 1.9)
    query_weight = gaussian(key_list[2], (D, INNER), D ** -0.5, 0.125, ((0, 64), (1, 8)))
    key_weight = gaussian(key_list[3], (D, INNER), D ** -0.5, 0.125, ((0, 64), (1, 8)))
    value_weight = gaussian(key_list[4], (D, INNER), D ** -0.5, 0.125, ((0, 64), (1, 8)))
    beta_weight = gaussian(key_list[5], (D, HEAD_COUNT), D ** -0.5, 0.125, ((0, 64), (1, 8)))
    decay_weight = gaussian(key_list[6], (D, HEAD_COUNT), D ** -0.5, 0.125, ((0, 64), (1, 8)))
    decay_rate = jnp.clip(jnp.exp(math.log(1.0) - 2.9957323 * jax.random.uniform(key_list[7], (HEAD_COUNT,), jnp.float32) ** levels(key_list[7], (HEAD_COUNT,), ((0, 8),), -0.2, 0.2)), 0.05, 1.0)
    prior_state = gaussian(key_list[8], (SEQUENCE_BATCH, HEAD_COUNT, HEAD_DIM, HEAD_DIM), 0.25, 1.5, ((0, 64), (1, 8)), jnp.float32)
    tail_keys = gaussian(key_list[9], (SEQUENCE_BATCH, HEAD_COUNT, PENDING_KEYS, HEAD_DIM), 1.0, 6.0, ((0, 64), (1, 8)))
    tail_values = gaussian(key_list[10], (SEQUENCE_BATCH, HEAD_COUNT, PENDING_KEYS, HEAD_DIM), 1.0, 6.0, ((0, 64), (1, 8)))
    tail_beta = jnp.clip(0.1 + 0.79999997 * jax.random.uniform(key_list[11], (SEQUENCE_BATCH, HEAD_COUNT, PENDING_KEYS), jnp.float32) ** levels(key_list[11], (SEQUENCE_BATCH, HEAD_COUNT, PENDING_KEYS), ((0, 64), (1, 8)), -0.2, 0.2), 0.1, 0.9)
    tail_decay = draw_tail_decay(jax.random.fold_in(key_list[18], 71), 0)
    lengths = ragged(key_list[13], SEQUENCE_BATCH, SEQUENCE_BATCH * PENDING_KEYS * 2 // 5, PENDING_KEYS, 2).astype(jnp.int32)
    out_weight = gaussian(key_list[14], (INNER, D), (INNER // 8) ** -0.5, 0.375, ((0, 8), (1, 64)))
    mlp_gain = jnp.clip(1.0 + 0.18 * jax.random.normal(key_list[15], (D,), jnp.float32), 0.1, 1.9)
    up_weight = gaussian(key_list[16], (D, FF), D ** -0.5, 0.125, ((0, 64), (1, 8)))
    down_weight = gaussian(key_list[17], (FF, D), FF ** -0.5, 0.0625, ((0, 8), (1, 64)))
    return dict(tokens=tokens, mix_gain=mix_gain, query_weight=query_weight, key_weight=key_weight, value_weight=value_weight, beta_weight=beta_weight, decay_weight=decay_weight, decay_rate=decay_rate, prior_state=prior_state, tail_keys=tail_keys, tail_values=tail_values, tail_beta=tail_beta, tail_decay=tail_decay, lengths=lengths, out_weight=out_weight, mlp_gain=mlp_gain, up_weight=up_weight, down_weight=down_weight)


epsilon = 1e-06

def unit_rows(vectors):
    return vectors * lax.rsqrt(lax.optimization_barrier(jnp.sum(vectors * vectors, axis=-1, keepdims=True)) + epsilon)

def delta_read(previous_state, keys, value_vectors, betas, decays, live_count, queries, new_key, new_value, new_beta, new_decay):
    peak_value = lax.Precision.HIGHEST
    positions = keys.shape[1]
    head_dim = keys.shape[2]
    live_mask = jnp.arange(positions, dtype=jnp.int32)[None, :] < live_count[:, None]
    unit_keys = unit_rows(keys.astype(jnp.float32))
    value_rows = value_vectors.astype(jnp.float32)
    beta_live = jnp.where(live_mask, betas, 0.0)
    decay_live = jnp.where(live_mask, decays, 0.0)
    cumulative = jnp.cumsum(decay_live, axis=1)
    row_index = jnp.arange(positions, dtype=jnp.int32)
    strict = (row_index[:, None] > row_index[None, :])[None]
    log_gap = cumulative[:, :, None] - cumulative[:, None, :]
    key_intersection = jnp.einsum('nik,njk->nij', unit_keys, unit_keys, precision=peak_value)
    lower_part = jnp.where(strict, beta_live[:, :, None] * jnp.exp(jnp.where(strict, log_gap, 0.0)) * key_intersection, 0.0)
    system = lower_part + jnp.eye(positions, dtype=jnp.float32)[None]
    right_sides = jnp.concatenate([(beta_live * jnp.exp(cumulative))[:, :, None] * unit_keys, beta_live[:, :, None] * value_rows], axis=2)
    solved = jax.scipy.linalg.solve_triangular(system, right_sides, lower=True, unit_diagonal=True)
    weight_matrix_rows = solved[:, :, :head_dim]
    unscaled_rows = solved[:, :, head_dim:]
    adjusted_result = unscaled_rows - jnp.einsum('mfd,mdx->mfx', weight_matrix_rows, previous_state, precision=peak_value)
    intersection = lax.optimization_barrier(jnp.sum(new_key * queries, axis=1))
    test_vector = queries - (new_beta * intersection)[:, None] * new_key
    total_decay = cumulative[:, -1]
    state_readout = jnp.einsum('rq,rqt->rt', test_vector, previous_state, precision=peak_value)
    tail_weights = jnp.exp(total_decay[:, None] - cumulative) * jnp.einsum('njk,nk->nj', unit_keys, test_vector, precision=peak_value)
    from_tail = jnp.einsum('nj,njv->nv', tail_weights, adjusted_result, precision=peak_value)
    readout = jnp.exp(total_decay)[:, None] * state_readout + from_tail
    return jnp.exp(new_decay)[:, None] * readout + (new_beta * intersection)[:, None] * new_value

def reference(tokens, mix_gain, query_weight, key_weight, value_weight, beta_weight, decay_weight, decay_rate, prior_state, tail_keys, tail_values, tail_beta, tail_decay, lengths, out_weight, mlp_gain, up_weight, down_weight):
    token_float = tokens.astype(jnp.float32)
    row_squares = lax.optimization_barrier(jnp.sum(token_float * token_float, axis=1, keepdims=True))
    row_scale = lax.rsqrt(row_squares / D + epsilon)
    normed = (token_float * mix_gain[None, :]).astype(jnp.bfloat16)

    def project(weight):
        return jnp.dot(normed.astype(jnp.float32), weight.astype(jnp.float32), preferred_element_type=jnp.float32) * row_scale

    def by_heads(raw):
        return raw.reshape(SEQUENCE_BATCH, HEAD_COUNT, HEAD_DIM)
    queries = unit_rows(jax.nn.silu(by_heads(project(query_weight))))
    new_keys = unit_rows(jax.nn.silu(by_heads(project(key_weight))))
    new_values = jax.nn.silu(by_heads(project(value_weight)))
    new_beta = jax.nn.sigmoid(project(beta_weight))
    new_decay = -decay_rate[None, :] * jax.nn.softplus(project(decay_weight))

    def one_head(operands):
        return delta_read(*operands)
    operands = (jnp.moveaxis(prior_state, 1, 0), jnp.moveaxis(tail_keys, 1, 0), jnp.moveaxis(tail_values, 1, 0), jnp.moveaxis(tail_beta, 1, 0), jnp.moveaxis(tail_decay, 1, 0), jnp.broadcast_to(lengths[None, :], (HEAD_COUNT, SEQUENCE_BATCH)), jnp.moveaxis(queries, 1, 0), jnp.moveaxis(new_keys, 1, 0), jnp.moveaxis(new_values, 1, 0), jnp.moveaxis(new_beta, 1, 0), jnp.moveaxis(new_decay, 1, 0))
    readout = jnp.moveaxis(lax.map(one_head, operands), 0, 1)
    head_out = readout.reshape(SEQUENCE_BATCH, INNER).astype(jnp.bfloat16)
    attended = jnp.dot(head_out.astype(jnp.float32), out_weight.astype(jnp.float32), preferred_element_type=jnp.float32)
    mixed_in = (token_float + attended).astype(jnp.bfloat16)
    mixed_float = mixed_in.astype(jnp.float32)
    mixer_squares = lax.optimization_barrier(jnp.sum(mixed_float * mixed_float, axis=1, keepdims=True))
    mixer_normed = (mixed_float * mlp_gain[None, :]).astype(jnp.bfloat16)
    hidden_raw = jnp.dot(mixer_normed.astype(jnp.float32), up_weight.astype(jnp.float32), preferred_element_type=jnp.float32) * lax.rsqrt(mixer_squares / D + epsilon)
    hidden = jnp.square(jnp.maximum(hidden_raw, 0.0)).astype(jnp.bfloat16)
    down = jnp.dot(hidden.astype(jnp.float32), down_weight.astype(jnp.float32), preferred_element_type=jnp.float32)
    return (mixed_float + down).astype(jnp.bfloat16)
```

```python
import jax
import jax.numpy as jnp
from jax import lax
from jax.experimental import pallas as pl
from jax.experimental.pallas import tpu as pltpu
from jax.sharding import PartitionSpec as P

D = 2048
N = 8
SEQ = 64
T_LEN = 64
epsilon = 1e-06
BF = jnp.bfloat16
F32 = jnp.float32
HI = lax.Precision.HIGHEST
MESH = pl.DeviceIdType.MESH

(TOK_A, TOK_B, W_Q, W_K, W_V, W_B, W_D, G_MIX, G_MLP, W_OUT, W_UP, W_DOWN,
 P_MAIN, P_AUX, HEADS, ATT, U_MAIN, U_AUX, HID, DOWN, FIN) = range(21)


def nt(a, b, precision=None):
    return lax.dot_general(a, b, (((1,), (1,)), ((), ())), preferred_element_type=F32, precision=precision)


def nn(a, b, precision=None):
    return lax.dot_general(a, b, (((1,), (0,)), ((), ())), preferred_element_type=F32, precision=precision)


def iota(shape, dim):
    return lax.broadcasted_iota(jnp.int32, shape, dim)


def split_rows(x):
    high = x.astype(BF)
    low = (x - high.astype(F32)).astype(BF)
    return jnp.concatenate([high.astype(F32), low.astype(F32)], axis=0).astype(BF)


def own_row(r):
    return jnp.sum(jnp.where(iota(r.shape, 0) == iota(r.shape, 1), r, 0.0), axis=0)


def rows_by(x, mats, contract):
    both = split_rows(x)
    lhs = jnp.broadcast_to(both[None], (N, *both.shape))
    r = lax.dot_general(lhs, mats, (((2,), (contract,)), ((0,), (0,))), preferred_element_type=F32)
    return own_row(r[:, :N] + r[:, N:])


def unit(x):
    return x * lax.rsqrt(jnp.sum(x * x, axis=-1, keepdims=True) + epsilon)


def silu(x):
    return x * (1.0 / (1.0 + jnp.exp(-x)))


def kernel(
    tok, mix_gain, wq, wk, wv, wb, wd, rate, state, tail_k, tail_v, tail_b, tail_g, lengths, wo, mlp_gain, wu, wdn,
    out,
    tok_a, x32, perm, xs, xt, xf, gq, gk, gv, gb, gd, ggm, ggl, go, gu, gdn, dperm, bd, gains,
    kbuf, vbuf, sbuf, sbf, tri, coef, pms, pmr, pxs, pxr, heads, att, mixed, mixt, ums, umr, uxs, uxr, hid, dns, dnr,
    fins, finr, flat, send_sem, recv_sem, local_sem,
):
    kv = lax.axis_index("kv")
    tp = lax.axis_index("tp")
    z = kv // N
    y = kv % N

    def peer(axis, r):
        if axis == "z":
            return (((z + r) % N) * N + y, tp)
        if axis == "y":
            return (z * N + (y + r) % N, tp)
        return (kv, (tp + r) % N)

    me = {"z": z, "y": y, "tp": tp}

    def copy(phase, axis, src, dst, r, slot, cut):
        return pltpu.make_async_remote_copy(
            src_ref=src.at[cut] if cut is not None else src,
            dst_ref=dst.at[slot],
            send_sem=send_sem.at[phase, r],
            recv_sem=recv_sem.at[phase, r],
            device_id=peer(axis, r),
            device_id_type=MESH,
        )

    plans = {}

    def send(phase, axis, src, dst, cut):
        plans[phase] = (axis, src, dst, cut)

        def step(r, _):
            where = (me[axis] + r) % N if cut == "peer" else (me[axis] if cut == "me" else None)
            copy(phase, axis, src, dst, r, me[axis], where).start()
            return 0

        lax.fori_loop(1, N, step, 0)

    def recv(phase):
        axis, src, dst, cut = plans[phase]

        def step(r, _):
            where = me[axis] if cut is not None else None
            copy(phase, axis, src, dst, r, (me[axis] - r + N) % N, where).wait_recv()
            return 0

        lax.fori_loop(1, N, step, 0)

    def sent(phase):
        axis, src, dst, cut = plans[phase]

        def step(r, _):
            where = me[axis] if cut is not None else None
            copy(phase, axis, src, dst, r, me[axis], where).wait_send()
            return 0

        lax.fori_loop(1, N, step, 0)

    loads = []
    for h in range(2):
        loads.append(pltpu.make_async_copy(tail_k.at[:, h], kbuf.at[h], local_sem.at[h]))
        loads.append(pltpu.make_async_copy(tail_v.at[:, h], vbuf.at[h], local_sem.at[2 + h]))
        loads.append(pltpu.make_async_copy(state.at[:, h], sbuf.at[h], local_sem.at[4 + h]))
    for load in loads:
        load.start()

    barrier = pltpu.get_barrier_semaphore()

    def greet(r, _):
        for axis in ("z", "y", "tp"):
            pl.semaphore_signal(barrier, inc=1, device_id=peer(axis, r), device_id_type=MESH)
        return 0

    lax.fori_loop(1, N, greet, 0)
    pl.semaphore_wait(barrier, 3 * (N - 1))

    send(TOK_A, "tp", tok, tok_a, None)
    send(G_MIX, "y", mix_gain, ggm, None)
    send(W_B, "y", wb, gb, None)
    send(W_D, "y", wd, gd, None)
    send(W_Q, "y", wq, gq, None)
    send(W_K, "y", wk, gk, None)

    tok_a[tp] = tok[...]
    ggm[y] = mix_gain[...]
    ggl[y] = mlp_gain[...]
    gb[y] = wb[...]
    gd[y] = wd[...]
    gq[y] = wq[...]
    gk[y] = wk[...]
    gv[y] = wv[...]
    go[y] = wo[...]
    gu[y] = wu[...]
    gdn[y] = wdn[...]
    bd[...] = jnp.zeros_like(bd)
    flat[...] = jnp.zeros_like(flat)
    row = iota((N * SEQ, N * SEQ), 0)
    column = iota((N * SEQ, N * SEQ), 1)
    swapped = (row // 64) * 8 + ((row // 8) % 8) * 64 + row % 8
    perm[...] = jnp.where(column == swapped, 1.0, 0.0).astype(BF)

    recv(TOK_A)
    for t in range(N):
        x32[4 * t : 4 * t + 4, :] = tok_a[t].astype(F32)
    arranged = nn(x32[...].astype(BF), perm[...])
    for t in range(N):
        xs[t] = arranged[:, 64 * t : 64 * t + 64].astype(BF)
    xt[y] = xs[y]
    send(TOK_B, "y", xs, xt, "peer")
    send(W_V, "y", wv, gv, None)
    send(G_MLP, "y", mlp_gain, ggl, None)
    send(W_OUT, "y", wo, go, None)
    send(W_UP, "y", wu, gu, None)
    send(W_DOWN, "y", wdn, gdn, None)

    for load in loads:
        load.wait()
    lens = jnp.zeros((N, T_LEN), jnp.int32)
    for i in range(N):
        lens = jnp.where(iota((N, T_LEN), 0) == i, lengths[i], lens)
    live = iota((N, T_LEN), 1) < lens
    upper = jnp.where(iota((T_LEN, T_LEN), 0) <= iota((T_LEN, T_LEN), 1), 1.0, 0.0)
    betas, gammas, totals, b3, g3, c3 = [], [], [], [], [], []
    for h in range(2):
        beta = jnp.where(live, tail_b[:, h, :], 0.0)
        decay = jnp.where(live, tail_g[:, h, :], 0.0)
        gamma = nn(decay, upper, HI)
        betas.append(beta)
        gammas.append(gamma)
        totals.append(jnp.sum(decay, axis=1, keepdims=True))
        b3.append(beta[:, None, :])
        g3.append(decay[:, None, :])
        c3.append(gamma[:, None, :])
    b3 = jnp.concatenate(b3, axis=0)
    g3 = jnp.concatenate(g3, axis=0)
    c3 = jnp.concatenate(c3, axis=0)
    keys = kbuf[...].reshape(2 * N, T_LEN, 128)
    gram = lax.dot_general(keys, keys, (((2,), (2,)), ((0,), (0,))), preferred_element_type=F32)
    i0 = iota((2 * N, T_LEN, T_LEN), 1)
    j0 = iota((2 * N, T_LEN, T_LEN), 2)
    diagonal = jnp.where(i0 == j0, gram, 0.0)
    inv_row = lax.rsqrt(jnp.sum(diagonal, axis=1, keepdims=True) + epsilon)
    inv_col = lax.rsqrt(jnp.sum(diagonal, axis=2, keepdims=True) + epsilon)
    gamma_col = jnp.sum(jnp.where(j0 <= i0, g3, 0.0), axis=2, keepdims=True)
    beta_col = jnp.sum(jnp.where(j0 == i0, b3, 0.0), axis=2, keepdims=True)
    below = i0 > j0
    lower = jnp.where(
        below, beta_col * jnp.exp(jnp.where(below, gamma_col - c3, 0.0)) * gram * inv_col * inv_row, 0.0
    )

    def part(m):
        return jnp.where((i0 // (2 * m) == j0 // (2 * m)) & (i0 // m != j0 // m), lower, 0.0)

    def bmm(a, b):
        return lax.dot_general(a, b, (((2,), (1,)), ((0,), (0,))), preferred_element_type=F32, precision=HI)

    inverse = jnp.where(i0 == j0, 1.0, 0.0) - part(1)
    for m in (2, 4, 8, 16, 32):
        inverse = inverse - bmm(bmm(inverse, part(m)), inverse)
    tri[...] = inverse
    for n in range(2 * N):
        coef[n : n + 1, :] = inv_row[n]
    sbf[...] = sbuf[...].astype(BF)

    for phase in (G_MIX, W_B, W_D, TOK_B):
        recv(phase)
    for t in range(N):
        gains[0:1, 32 * t : 32 * t + 32] = ggm[t]
        bd[0:2, 32 * t : 32 * t + 32] = gb[t].astype(F32)
        bd[2:4, 32 * t : 32 * t + 32] = gd[t].astype(F32)
    eye64 = jnp.where(iota((SEQ, SEQ), 0) == iota((SEQ, SEQ), 1), 1.0, 0.0).astype(BF)
    token = nt(eye64, xt[...].reshape(256, SEQ))
    xf[...] = token
    squares = jnp.sum(token * token, axis=1, keepdims=True)
    normed = (token * gains[0:1, :]).astype(BF)
    aux = nt(normed, bd[...].astype(BF))
    pxs[...] = jnp.where(iota((SEQ, 128), 1) == 4, squares, aux).reshape(N, N, 128)
    pxr[z] = pxs[z]
    send(P_AUX, "z", pxs, pxr, "peer")
    for at, (phase, w) in enumerate(((W_Q, gq), (W_K, gk), (W_V, gv))):
        recv(phase)
        pms[:, :, 256 * at : 256 * at + 256] = (
            nn(normed, w[...].reshape(256, 256)).reshape(N, N, 256).astype(BF)
        )
    pmr[z] = pms[z]
    send(P_MAIN, "z", pms, pmr, "peer")

    recv(P_AUX)
    aux = jnp.sum(pxr[...], axis=0)
    row_scale = lax.rsqrt(aux[:, 4:5] / D + epsilon)
    recv(P_MAIN)
    raw = jnp.sum(pmr[...].astype(F32), axis=0) * row_scale
    results = []
    for h in range(2):
        query = unit(silu(raw[:, 128 * h : 128 * h + 128]))
        key = unit(silu(raw[:, 256 + 128 * h : 384 + 128 * h]))
        value = silu(raw[:, 512 + 128 * h : 640 + 128 * h])
        new_beta = 1.0 / (1.0 + jnp.exp(-(aux[:, h : h + 1] * row_scale)))
        pre = aux[:, 2 + h : 3 + h] * row_scale
        soft = jnp.maximum(pre, 0.0) + jnp.log(1.0 + jnp.exp(-jnp.abs(pre)))
        new_decay = -rate[h] * soft
        weight = new_beta * jnp.sum(key * query, axis=1, keepdims=True)
        test = query - weight * key
        inv = coef[N * h : N * h + N, :]
        a = rows_by(test, kbuf[h], 2) * jnp.exp(totals[h] - gammas[h]) * inv
        lhs = jnp.broadcast_to(a[None], (N, N, T_LEN))
        solved = own_row(bmm(lhs, tri[N * h : N * h + N])) * betas[h]
        from_values = rows_by(solved, vbuf[h], 1)
        moved = jnp.exp(totals[h]) * test - rows_by(solved * jnp.exp(gammas[h]) * inv, kbuf[h], 1)
        readout = rows_by(moved, sbf[h], 1) + from_values
        results.append(jnp.exp(new_decay) * readout + weight * value)
    heads[z] = jnp.concatenate(results, axis=1).astype(BF)
    send(HEADS, "z", heads, heads, "me")

    recv(W_OUT)
    recv(G_MLP)
    for t in range(N):
        gains[1:2, 32 * t : 32 * t + 32] = ggl[t]
    recv(HEADS)
    gathered = heads[...].astype(F32).reshape(SEQ, 256).astype(BF)
    att[tp] = nt(gathered, go[...].reshape(256, 256)).astype(BF)
    send(ATT, "tp", att, att, "me")
    r0 = iota((256, 256), 0)
    r1 = iota((256, 256), 1)
    regroup = jnp.where(r1 == ((r0 // 4) % 8) * 32 + (r0 // 32) * 4 + r0 % 4, 1.0, 0.0).astype(BF)
    recv(W_UP)
    recv(ATT)
    mixed[...] = (xf[...] + jnp.sum(att[...].astype(F32), axis=0)).astype(BF)
    mixer = mixed[...].astype(F32)
    squares = jnp.sum(mixer * mixer, axis=1, keepdims=True)
    uxs[...] = jnp.broadcast_to(squares, (SEQ, 128)).reshape(N, N, 128)
    uxr[z] = uxs[z]
    send(U_AUX, "z", uxs, uxr, "peer")
    normed = (mixer * gains[1:2, :]).astype(BF)
    ums[...] = nn(normed, gu[...].reshape(256, 1024)).reshape(N, N, 1024).astype(BF)
    umr[z] = ums[z]
    send(U_MAIN, "z", ums, umr, "peer")
    mixt[...] = nt(regroup, mixed[...]).reshape(N, 32, SEQ)
    recv(U_AUX)
    row_scale = lax.rsqrt(jnp.sum(uxr[...], axis=0)[:, 0:1] / D + epsilon)
    recv(U_MAIN)
    raw = jnp.maximum(jnp.sum(umr[...].astype(F32), axis=0) * row_scale, 0.0)
    hid[z] = (raw * raw).astype(BF)
    send(HID, "z", hid, hid, "me")
    recv(W_DOWN)
    dperm[...] = nn(regroup, gdn[...].reshape(256, 1024)).astype(BF)
    recv(HID)
    hidden = hid[...].astype(F32).reshape(SEQ, 1024).astype(BF)
    dns[...] = nt(dperm[...], hidden).reshape(N, 32, SEQ).astype(BF)
    dnr[tp] = dns[tp]
    send(DOWN, "tp", dns, dnr, "peer")
    recv(DOWN)
    total = mixt[tp] + jnp.sum(dnr[...].astype(F32), axis=0)
    for t in range(N):
        fins[t] = total[4 * t : 4 * t + 4, :].astype(BF)
    finr[y] = fins[y]
    send(FIN, "y", fins, finr, "peer")
    recv(FIN)
    for t in range(N):
        flat[0:4, 64 * t : 64 * t + 64] = finr[t].astype(F32)
    out[...] = nn(flat[...].astype(BF), perm[...])[0:4, :].astype(BF)
    for phase in sorted(plans):
        sent(phase)


def local(
    tokens, mix_gain, query_weight, key_weight, value_weight, beta_weight, decay_weight, decay_rate, prior_state,
    tail_keys, tail_values, tail_beta, tail_decay, lengths, out_weight, mlp_gain, up_weight, down_weight,
):
    vmem = pl.BlockSpec(memory_space=pltpu.VMEM)
    smem = pl.BlockSpec(memory_space=pltpu.SMEM)
    hbm = pl.BlockSpec(memory_space=pl.ANY)
    specs = [vmem] * 7 + [smem] + [hbm] * 3 + [vmem] * 2 + [smem] + [vmem] * 4

    def v(*shape, dtype=BF):
        return pltpu.VMEM(shape, dtype)

    result = pl.pallas_call(
        kernel,
        out_shape=jax.ShapeDtypeStruct((4, 512), BF),
        in_specs=specs,
        out_specs=vmem,
        scratch_shapes=[
            v(8, 4, 512), v(32, 512, dtype=F32), v(512, 512), v(8, 32, 64), v(8, 32, 64), v(64, 256, dtype=F32),
            v(8, 32, 256), v(8, 32, 256), v(8, 32, 256), v(8, 2, 32), v(8, 2, 32),
            v(8, 1, 32, dtype=F32), v(8, 1, 32, dtype=F32),
            v(8, 32, 256), v(8, 32, 1024), v(8, 32, 1024), v(256, 1024), v(128, 256, dtype=F32), v(8, 256, dtype=F32),
            v(2, 8, 64, 128), v(2, 8, 64, 128), v(2, 8, 128, 128, dtype=F32), v(2, 8, 128, 128),
            v(16, 64, 64, dtype=F32), v(16, 64, dtype=F32),
            v(8, 8, 768), v(8, 8, 768), v(8, 8, 128, dtype=F32), v(8, 8, 128, dtype=F32),
            v(8, 8, 256), v(8, 64, 256), v(64, 256), v(8, 32, 64, dtype=F32),
            v(8, 8, 1024), v(8, 8, 1024), v(8, 8, 128, dtype=F32), v(8, 8, 128, dtype=F32),
            v(8, 8, 1024), v(8, 32, 64), v(8, 32, 64), v(8, 4, 64), v(8, 4, 64), v(8, 512, dtype=F32),
            pltpu.SemaphoreType.DMA((21, 8)), pltpu.SemaphoreType.DMA((21, 8)), pltpu.SemaphoreType.DMA((6,)),
        ],
        compiler_params=pltpu.CompilerParams(collective_id=0, has_side_effects=True),
    )(
        tokens.T, mix_gain.reshape(1, -1), query_weight, key_weight, value_weight, beta_weight.T, decay_weight.T,
        decay_rate, prior_state, tail_keys, tail_values, tail_beta, tail_decay, lengths, out_weight.T,
        mlp_gain.reshape(1, -1), up_weight, down_weight.T,
    )
    return result.T


def solution(mesh):
    kt = ("kv", "tp")
    return jax.shard_map(
        local,
        mesh=mesh,
        in_specs=(
            P(None, kt), P("kv"), P("kv", "tp"), P("kv", "tp"), P("kv", "tp"), P("kv", "tp"), P("kv", "tp"), P("tp"),
            P("kv", "tp", None, None), P("kv", "tp", None, None), P("kv", "tp", None, None),
            P("kv", "tp", None), P("kv", "tp", None), P("kv"), P("tp", "kv"), P("kv"), P("kv", "tp"), P("tp", "kv"),
        ),
        out_specs=P(None, kt),
        check_vma=False,
    )
```

```python
import jax
import jax.numpy as jnp
from jax import lax
from jax.experimental import pallas as pl
from jax.experimental.pallas import tpu as pltpu
from jax.sharding import PartitionSpec as P

D = 2048
N = 8
SEQ = 64
T_LEN = 64
epsilon = 1e-06
BF = jnp.bfloat16
F32 = jnp.float32
HI = lax.Precision.HIGHEST
MESH = pl.DeviceIdType.MESH

(TOK_A, TOK_Y, TOK_Z, W_Y, W_Z, W_B, W_D, G_MIX, G_MIZ, G_MLP, W_OUT, W_UP, W_UP2, W_DOWN, W_DOWN2,
 P_Y, P_Z, P_AUX, HEADS, ATT, U_MAIN, U_AUX, HID, DOWN, FIN) = range(25)
FAR_FIRST = (4, 3, 5, 2, 6, 1, 7)


def nt(a, b, precision=None):
    return lax.dot_general(a, b, (((1,), (1,)), ((), ())), preferred_element_type=F32, precision=precision)


def nn(a, b, precision=None):
    return lax.dot_general(a, b, (((1,), (0,)), ((), ())), preferred_element_type=F32, precision=precision)


def iota(shape, dim):
    return lax.broadcasted_iota(jnp.int32, shape, dim)


def split_rows(x):
    high = x.astype(BF)
    low = (x - high.astype(F32)).astype(BF)
    return jnp.concatenate([high.astype(F32), low.astype(F32)], axis=0).astype(BF)


def own_row(r):
    return jnp.sum(jnp.where(iota(r.shape, 0) == iota(r.shape, 1), r, 0.0), axis=0)


def rows_by(x, mats, contract):
    both = split_rows(x)
    lhs = jnp.broadcast_to(both[None], (N, *both.shape))
    r = lax.dot_general(lhs, mats, (((2,), (contract,)), ((0,), (0,))), preferred_element_type=F32)
    return own_row(r[:, :N] + r[:, N:])


def unit(x):
    return x * lax.rsqrt(jnp.sum(x * x, axis=-1, keepdims=True) + epsilon)


def silu(x):
    return x * (1.0 / (1.0 + jnp.exp(-x)))


def kernel(
    tok, mix_gain, wq, wk, wv, wb, wd, rate, state, tail_k, tail_v, tail_b, tail_g, lengths, wo, mlp_gain, wu, wdn,
    out,
    tok_a, x32, perm, xs, xt, xzs, xzt, xf, gy, gz, gb, gd, ggm, ggz, ggl, go, gu, gdn, dperm, bd, gains,
    kbuf, vbuf, sbuf, sbf, tbb, tgg, tri, coef, pys, pyr, pzs, pzr, pxs, pxr, heads, att, mixed, mixt,
    ums, umr, uxs, uxr, hid, dns, dnr, fins, finr, flat, send_sem, recv_sem, local_sem,
):
    kv = lax.axis_index("kv")
    tp = lax.axis_index("tp")
    z = kv // N
    y = kv % N

    def peer(axis, r):
        if axis == "z":
            return (((z + r) % N) * N + y, tp)
        if axis == "y":
            return (z * N + (y + r) % N, tp)
        return (kv, (tp + r) % N)

    me = {"z": z, "y": y, "tp": tp}
    started = []

    def copy(phase, axis, src, dst, r):
        pltpu.make_async_remote_copy(
            src_ref=src,
            dst_ref=dst,
            send_sem=send_sem.at[phase],
            recv_sem=recv_sem.at[phase],
            device_id=peer(axis, r),
            device_id_type=MESH,
        ).start()

    def gather(phase, axis, buf, steps=FAR_FIRST):
        started.append((phase, buf, len(steps)))
        for r in steps:
            copy(phase, axis, buf.at[me[axis]], buf.at[me[axis]], r)

    def scatter(phase, axis, src, dst):
        started.append((phase, dst, N - 1))
        for r in FAR_FIRST:
            copy(phase, axis, src.at[(me[axis] + r) % N], dst.at[me[axis]], r)

    def relay(phase, axis, buf):
        started.append((phase, buf, 3))
        behind, ahead = (me[axis] + N - 2) % N, (me[axis] + 2) % N
        copy(phase, axis, buf.at[behind], buf.at[behind], 2)
        copy(phase, axis, buf.at[behind], buf.at[behind], 1)
        copy(phase, axis, buf.at[ahead], buf.at[ahead], 7)

    def recv(phase):
        for p, buf, count in started:
            if p == phase:
                part = buf.at[pl.ds(0, count)]
                pltpu.make_async_copy(part, part, recv_sem.at[phase]).wait()

    loads = {}

    def load(name, src, dst):
        c = pltpu.make_async_copy(src, dst, local_sem.at[len(loads)])
        c.start()
        loads[name] = c

    load("tok", tok, tok_a.at[tp])
    load("mix", mix_gain, ggm.at[y])
    load("miz", mix_gain, ggz.at[z])
    load("b", wb, gb.at[y])
    load("d", wd, gd.at[y])
    load("q", wq, gy.at[y, :, pl.ds(0, 256)])
    load("k0", wk.at[:, pl.ds(0, 128)], gy.at[y, :, pl.ds(256, 128)])
    load("k1", wk.at[:, pl.ds(128, 128)], gz.at[z, :, pl.ds(0, 128)])
    load("v", wv, gz.at[z, :, pl.ds(128, 256)])
    load("mlp", mlp_gain, ggl.at[y])
    load("out", wo, go.at[y])
    load("up", wu, gu.at[y])
    load("down", wdn, gdn.at[y])
    load("tb", tail_b, tbb)
    load("tg", tail_g, tgg)
    for h in range(2):
        load(("tk", h), tail_k.at[:, h], kbuf.at[h])
        load(("ts", h), state.at[:, h], sbuf.at[h])
        load(("tv", h), tail_v.at[:, h], vbuf.at[h])

    barrier = pltpu.get_barrier_semaphore()
    for r in FAR_FIRST:
        for axis in ("z", "y", "tp"):
            pl.semaphore_signal(barrier, inc=1, device_id=peer(axis, r), device_id_type=MESH)

    bd[...] = jnp.zeros_like(bd)
    flat[...] = jnp.zeros_like(flat)
    row = iota((N * SEQ, N * SEQ), 0)
    column = iota((N * SEQ, N * SEQ), 1)
    swapped = (row // 64) * 8 + ((row // 8) % 8) * 64 + row % 8
    perm[...] = jnp.where(column == swapped, 1.0, 0.0).astype(BF)
    for name in loads:
        loads[name].wait()

    pl.semaphore_wait(barrier, 3 * (N - 1))

    gather(TOK_A, "tp", tok_a)
    gather(G_MIX, "y", ggm)
    gather(W_B, "y", gb)
    gather(W_D, "y", gd)
    gather(G_MIZ, "z", ggz)
    gather(W_Y, "y", gy)
    gather(W_Z, "z", gz)
    gather(G_MLP, "y", ggl)

    lens = jnp.zeros((N, T_LEN), jnp.int32)
    for i in range(N):
        lens = jnp.where(iota((N, T_LEN), 0) == i, lengths[i], lens)
    live = iota((N, T_LEN), 1) < lens
    upper = jnp.where(iota((T_LEN, T_LEN), 0) <= iota((T_LEN, T_LEN), 1), 1.0, 0.0)
    betas, gammas, totals, b3, g3, c3 = [], [], [], [], [], []
    for h in range(2):
        beta = jnp.where(live, tbb[:, h, :], 0.0)
        decay = jnp.where(live, tgg[:, h, :], 0.0)
        gamma = nn(decay, upper, HI)
        betas.append(beta)
        gammas.append(gamma)
        totals.append(jnp.sum(decay, axis=1, keepdims=True))
        b3.append(beta[:, None, :])
        g3.append(decay[:, None, :])
        c3.append(gamma[:, None, :])
    b3 = jnp.concatenate(b3, axis=0)
    g3 = jnp.concatenate(g3, axis=0)
    c3 = jnp.concatenate(c3, axis=0)
    keys = kbuf[...].reshape(2 * N, T_LEN, 128)
    gram = lax.dot_general(keys, keys, (((2,), (2,)), ((0,), (0,))), preferred_element_type=F32)
    i0 = iota((2 * N, T_LEN, T_LEN), 1)
    j0 = iota((2 * N, T_LEN, T_LEN), 2)
    diagonal = jnp.where(i0 == j0, gram, 0.0)
    inv_row = lax.rsqrt(jnp.sum(diagonal, axis=1, keepdims=True) + epsilon)
    inv_col = lax.rsqrt(jnp.sum(diagonal, axis=2, keepdims=True) + epsilon)
    gamma_col = jnp.sum(jnp.where(j0 <= i0, g3, 0.0), axis=2, keepdims=True)
    beta_col = jnp.sum(jnp.where(j0 == i0, b3, 0.0), axis=2, keepdims=True)
    below = i0 > j0
    lower = jnp.where(
        below, beta_col * jnp.exp(jnp.where(below, gamma_col - c3, 0.0)) * gram * inv_col * inv_row, 0.0
    )
    for n in range(2 * N):
        coef[n : n + 1, :] = inv_row[n]
    tri[...] = lower
    sbf[...] = sbuf[...].astype(BF)

    recv(TOK_A)
    for t in range(N):
        x32[4 * t : 4 * t + 4, :] = tok_a[t].astype(F32)
    whole = x32[...].astype(BF)
    arranged = nn(whole, perm[...])
    for t in range(N):
        xs[t] = arranged[:, 64 * t : 64 * t + 64].astype(BF)
        xzs[t] = x32[:, 64 * t : 64 * t + 64].astype(BF)
    xt[y] = xs[y]
    xzt[z] = xzs[z]
    scatter(TOK_Y, "y", xs, xt)
    scatter(TOK_Z, "z", xzs, xzt)
    gather(W_UP, "y", gu, (2, 6, 1, 7))

    def part(m):
        return jnp.where((i0 // (2 * m) == j0 // (2 * m)) & (i0 // m != j0 // m), tri[...], 0.0)

    def bmm(a, b):
        return lax.dot_general(a, b, (((2,), (1,)), ((0,), (0,))), preferred_element_type=F32, precision=HI)

    inverse = jnp.where(i0 == j0, 1.0, 0.0) - part(1)
    for m in (2, 4, 8, 16, 32):
        inverse = inverse - bmm(bmm(inverse, part(m)), inverse)
    tri[...] = inverse

    for phase in (G_MIX, G_MIZ, W_B, W_D):
        recv(phase)
    for t in range(N):
        gains[0:1, 32 * t : 32 * t + 32] = ggm[t]
        gains[1:2, 32 * t : 32 * t + 32] = ggz[t]
        bd[0:2, 32 * t : 32 * t + 32] = gb[t].astype(F32)
        bd[2:4, 32 * t : 32 * t + 32] = gd[t].astype(F32)
    eye64 = jnp.where(iota((SEQ, SEQ), 0) == iota((SEQ, SEQ), 1), 1.0, 0.0).astype(BF)
    recv(TOK_Y)
    token = nt(eye64, xt[...].reshape(256, SEQ))
    xf[...] = token
    squares = jnp.sum(token * token, axis=1, keepdims=True)
    normed = (token * gains[0:1, :]).astype(BF)
    aux = nt(normed, bd[...].astype(BF))
    pxs[...] = jnp.where(iota((SEQ, 128), 1) == 4, squares, aux).reshape(N, N, 128)
    pxr[z] = pxs[z]
    scatter(P_AUX, "z", pxs, pxr)
    recv(W_Y)
    pys[...] = nn(normed, gy[...].reshape(256, 384)).reshape(N, N, 384).astype(BF)
    pyr[z] = pys[z]
    scatter(P_Y, "z", pys, pyr)
    recv(TOK_Z)
    other = (nt(eye64, xzt[...].reshape(256, SEQ)) * gains[1:2, :]).astype(BF)
    recv(W_Z)
    pzs[...] = nn(other, gz[...].reshape(256, 384)).reshape(N, N, 384).astype(BF)
    pzr[y] = pzs[y]
    scatter(P_Z, "y", pzs, pzr)
    gather(W_OUT, "y", go)
    r0 = iota((256, 256), 0)
    r1 = iota((256, 256), 1)
    regroup = jnp.where(r1 == ((r0 // 4) % 8) * 32 + (r0 // 32) * 4 + r0 % 4, 1.0, 0.0).astype(BF)

    recv(W_UP)
    relay(W_UP2, "y", gu)
    gather(W_DOWN, "y", gdn, (2, 6, 1, 7))
    recv(P_AUX)
    aux = jnp.sum(pxr[...], axis=0)
    row_scale = lax.rsqrt(aux[:, 4:5] / D + epsilon)
    recv(P_Y)
    raw_y = jnp.sum(pyr[...].astype(F32), axis=0) * row_scale
    recv(P_Z)
    raw_z = jnp.sum(pzr[...].astype(F32), axis=0) * row_scale
    results = []
    for h in range(2):
        query = unit(silu(raw_y[:, 128 * h : 128 * h + 128]))
        key = unit(silu(raw_y[:, 256:384] if h == 0 else raw_z[:, 0:128]))
        value = silu(raw_z[:, 128 + 128 * h : 256 + 128 * h])
        new_beta = 1.0 / (1.0 + jnp.exp(-(aux[:, h : h + 1] * row_scale)))
        pre = aux[:, 2 + h : 3 + h] * row_scale
        soft = jnp.maximum(pre, 0.0) + jnp.log(1.0 + jnp.exp(-jnp.abs(pre)))
        new_decay = -rate[h] * soft
        weight = new_beta * jnp.sum(key * query, axis=1, keepdims=True)
        test = query - weight * key
        inv = coef[N * h : N * h + N, :]
        a = rows_by(test, kbuf[h], 2) * jnp.exp(totals[h] - gammas[h]) * inv
        lhs = jnp.broadcast_to(a[None], (N, N, T_LEN))
        solved = own_row(bmm(lhs, tri[N * h : N * h + N])) * betas[h]
        from_values = rows_by(solved, vbuf[h], 1)
        moved = jnp.exp(totals[h]) * test - rows_by(solved * jnp.exp(gammas[h]) * inv, kbuf[h], 1)
        readout = rows_by(moved, sbf[h], 1) + from_values
        results.append(jnp.exp(new_decay) * readout + weight * value)
    heads[z] = jnp.concatenate(results, axis=1).astype(BF)
    gather(HEADS, "z", heads)

    recv(W_OUT)
    recv(G_MLP)
    for t in range(N):
        gains[2:3, 32 * t : 32 * t + 32] = ggl[t]
    recv(HEADS)
    gathered = heads[...].astype(F32).reshape(SEQ, 256).astype(BF)
    att[tp] = nt(gathered, go[...].reshape(256, 256)).astype(BF)
    gather(ATT, "tp", att)
    recv(W_DOWN)
    relay(W_DOWN2, "y", gdn)
    recv(W_UP2)
    recv(ATT)
    mixed[...] = (xf[...] + jnp.sum(att[...].astype(F32), axis=0)).astype(BF)
    mixer = mixed[...].astype(F32)
    normed = (mixer * gains[2:3, :]).astype(BF)
    ums[...] = nn(normed, gu[...].reshape(256, 1024)).reshape(N, N, 1024).astype(BF)
    umr[z] = ums[z]
    scatter(U_MAIN, "z", ums, umr)
    squares = jnp.sum(mixer * mixer, axis=1, keepdims=True)
    uxs[...] = jnp.broadcast_to(squares, (SEQ, 128)).reshape(N, N, 128)
    uxr[z] = uxs[z]
    scatter(U_AUX, "z", uxs, uxr)
    mixt[...] = nt(regroup, mixed[...]).reshape(N, 32, SEQ)
    recv(U_MAIN)
    raw = jnp.sum(umr[...].astype(F32), axis=0)
    recv(U_AUX)
    row_scale = lax.rsqrt(jnp.sum(uxr[...], axis=0)[:, 0:1] / D + epsilon)
    raw = jnp.maximum(raw * row_scale, 0.0)
    hid[z] = (raw * raw).astype(BF)
    gather(HID, "z", hid)
    recv(W_DOWN2)
    dperm[...] = nn(regroup, gdn[...].reshape(256, 1024)).astype(BF)
    recv(HID)
    hidden = hid[...].astype(F32).reshape(SEQ, 1024).astype(BF)
    dns[...] = nt(dperm[...], hidden).reshape(N, 32, SEQ).astype(BF)
    dnr[tp] = dns[tp]
    scatter(DOWN, "tp", dns, dnr)
    recv(DOWN)
    total = mixt[tp] + jnp.sum(dnr[...].astype(F32), axis=0)
    for t in range(N):
        fins[t] = total[4 * t : 4 * t + 4, :].astype(BF)
    finr[y] = fins[y]
    scatter(FIN, "y", fins, finr)
    for phase, buf, count in started[:-1]:
        part_of = buf.at[pl.ds(0, count)]
        pltpu.make_async_copy(part_of, part_of, send_sem.at[phase]).wait()
    recv(FIN)
    for t in range(N):
        flat[0:4, 64 * t : 64 * t + 64] = finr[t].astype(F32)
    out[...] = nn(flat[...].astype(BF), perm[...])[0:4, :].astype(BF)
    last = finr.at[pl.ds(0, N - 1)]
    pltpu.make_async_copy(last, last, send_sem.at[FIN]).wait()


def local(
    tokens, mix_gain, query_weight, key_weight, value_weight, beta_weight, decay_weight, decay_rate, prior_state,
    tail_keys, tail_values, tail_beta, tail_decay, lengths, out_weight, mlp_gain, up_weight, down_weight,
):
    vmem = pl.BlockSpec(memory_space=pltpu.VMEM)
    smem = pl.BlockSpec(memory_space=pltpu.SMEM)
    hbm = pl.BlockSpec(memory_space=pl.ANY)
    specs = [hbm] * 7 + [smem] + [hbm] * 5 + [smem] + [hbm] * 4

    def v(*shape, dtype=BF):
        return pltpu.VMEM(shape, dtype)

    def f(*shape):
        return v(*shape, dtype=F32)

    result = pl.pallas_call(
        kernel,
        out_shape=jax.ShapeDtypeStruct((4, 512), BF),
        in_specs=specs,
        out_specs=vmem,
        scratch_shapes=[
            v(8, 4, 512), f(32, 512), v(512, 512), v(8, 32, 64), v(8, 32, 64), v(8, 32, 64), v(8, 32, 64), f(64, 256),
            v(8, 32, 384), v(8, 32, 384), v(8, 2, 32), v(8, 2, 32), f(8, 1, 32), f(8, 1, 32), f(8, 1, 32),
            v(8, 32, 256), v(8, 32, 1024), v(8, 32, 1024), v(256, 1024), f(128, 256), f(8, 256),
            v(2, 8, 64, 128), v(2, 8, 64, 128), f(2, 8, 128, 128), v(2, 8, 128, 128), f(8, 2, 64), f(8, 2, 64),
            f(16, 64, 64), f(16, 64),
            v(8, 8, 384), v(8, 8, 384), v(8, 8, 384), v(8, 8, 384), f(8, 8, 128), f(8, 8, 128),
            v(8, 8, 256), v(8, 64, 256), v(64, 256), f(8, 32, 64),
            v(8, 8, 1024), v(8, 8, 1024), f(8, 8, 128), f(8, 8, 128),
            v(8, 8, 1024), v(8, 32, 64), v(8, 32, 64), v(8, 4, 64), v(8, 4, 64), f(8, 512),
            pltpu.SemaphoreType.DMA((25,)), pltpu.SemaphoreType.DMA((25,)), pltpu.SemaphoreType.DMA((21,)),
        ],
        compiler_params=pltpu.CompilerParams(collective_id=0, has_side_effects=True),
    )(
        tokens.T, mix_gain.reshape(1, -1), query_weight, key_weight, value_weight, beta_weight.T, decay_weight.T,
        decay_rate, prior_state, tail_keys, tail_values, tail_beta, tail_decay, lengths, out_weight.T,
        mlp_gain.reshape(1, -1), up_weight, down_weight.T,
    )
    return result.T


def solution(mesh):
    kt = ("kv", "tp")
    return jax.shard_map(
        local,
        mesh=mesh,
        in_specs=(
            P(None, kt), P("kv"), P("kv", "tp"), P("kv", "tp"), P("kv", "tp"), P("kv", "tp"), P("kv", "tp"), P("tp"),
            P("kv", "tp", None, None), P("kv", "tp", None, None), P("kv", "tp", None, None),
            P("kv", "tp", None), P("kv", "tp", None), P("kv"), P("tp", "kv"), P("kv"), P("kv", "tp"), P("tp", "kv"),
        ),
        out_specs=P(None, kt),
        check_vma=False,
    )
```

```python
import jax
import jax.numpy as jnp
from jax import lax
from jax.experimental import pallas as pl
from jax.experimental.pallas import tpu as pltpu
from jax.sharding import PartitionSpec as P

D = 2048
N = 8
SEQ = 64
T_LEN = 64
epsilon = 1e-06
BF = jnp.bfloat16
F32 = jnp.float32
HI = lax.Precision.HIGHEST
MESH = pl.DeviceIdType.MESH

(TOK_A, TOK_Y, TOK_Z, W_Y, W_Z, W_B, W_D, G_MIX, G_MIZ, G_MLP, W_OUT, W_OUT2, W_UP, W_UP2, W_DOWN, W_DOWN2,
 P_Y, P_Z, HEADS, ATT, U_MAIN, HID, DOWN) = range(23)
FAR_FIRST = (4, 3, 5, 2, 6, 1, 7)


def nt(a, b, precision=None):
    return lax.dot_general(a, b, (((1,), (1,)), ((), ())), preferred_element_type=F32, precision=precision)


def nn(a, b, precision=None):
    return lax.dot_general(a, b, (((1,), (0,)), ((), ())), preferred_element_type=F32, precision=precision)


def iota(shape, dim):
    return lax.broadcasted_iota(jnp.int32, shape, dim)


def split_rows(x):
    high = x.astype(BF)
    low = (x - high.astype(F32)).astype(BF)
    return jnp.concatenate([high.astype(F32), low.astype(F32)], axis=0).astype(BF)


def own_row(r):
    return jnp.sum(jnp.where(iota(r.shape, 0) == iota(r.shape, 1), r, 0.0), axis=0)


def rows_by(x, mats, contract):
    both = split_rows(x)
    lhs = jnp.broadcast_to(both[None], (N, *both.shape))
    r = lax.dot_general(lhs, mats, (((2,), (contract,)), ((0,), (0,))), preferred_element_type=F32)
    return own_row(r[:, :N] + r[:, N:])


def unit(x):
    return x * lax.rsqrt(jnp.sum(x * x, axis=-1, keepdims=True) + epsilon)


def silu(x):
    return x * (1.0 / (1.0 + jnp.exp(-x)))


def kernel(
    tok, mix_gain, wq, wk, wv, wb, wd, rate, state, tail_k, tail_v, tail_b, tail_g, lengths, wo, mlp_gain, wu, wdn,
    out,
    tok_a, x32, perm, xs, xt, xzs, xzt, xf, gy, gz, gb, gd, ggm, ggz, ggl, go, gu, gdn, bd, gains,
    kbuf, vbuf, sbuf, sbf, tbb, tgg, tri, coef, pys, pyr, pzs, pzr, heads, att, mixed, mixt,
    ums, umr, hid, down_t, dns, dnr, flat, send_sem, recv_sem, local_sem,
):
    kv = lax.axis_index("kv")
    tp = lax.axis_index("tp")
    z = kv // N
    y = kv % N

    def peer(axis, r):
        if axis == "z":
            return (((z + r) % N) * N + y, tp)
        if axis == "y":
            return (z * N + (y + r) % N, tp)
        return (kv, (tp + r) % N)

    me = {"z": z, "y": y, "tp": tp}
    started = []

    def copy(phase, axis, src, dst, r):
        pltpu.make_async_remote_copy(
            src_ref=src,
            dst_ref=dst,
            send_sem=send_sem.at[phase],
            recv_sem=recv_sem.at[phase],
            device_id=peer(axis, r),
            device_id_type=MESH,
        ).start()

    def gather(phase, axis, buf, steps=FAR_FIRST):
        started.append((phase, buf, len(steps)))
        for r in steps:
            copy(phase, axis, buf.at[me[axis]], buf.at[me[axis]], r)

    def scatter(phase, axis, src, dst):
        started.append((phase, dst, N - 1))
        for r in FAR_FIRST:
            copy(phase, axis, src.at[(me[axis] + r) % N], dst.at[me[axis]], r)

    def relay(phase, axis, buf):
        started.append((phase, buf, 3))
        behind, ahead = (me[axis] + N - 2) % N, (me[axis] + 2) % N
        copy(phase, axis, buf.at[behind], buf.at[behind], 2)
        copy(phase, axis, buf.at[behind], buf.at[behind], 1)
        copy(phase, axis, buf.at[ahead], buf.at[ahead], 7)

    def recv(phase):
        for p, buf, count in started:
            if p == phase:
                part = buf.at[pl.ds(0, count)]
                pltpu.make_async_copy(part, part, recv_sem.at[phase]).wait()

    barrier = pltpu.get_barrier_semaphore()
    for r in FAR_FIRST:
        for axis in ("z", "y", "tp"):
            pl.semaphore_signal(barrier, inc=1, device_id=peer(axis, r), device_id_type=MESH)

    loads = {}

    def load(name, src, dst):
        c = pltpu.make_async_copy(src, dst, local_sem.at[len(loads)])
        c.start()
        loads[name] = c

    load("tok", tok, tok_a.at[tp])
    load("mix", mix_gain, ggm.at[y])
    load("miz", mix_gain, ggz.at[z])
    load("b", wb, gb.at[y])
    load("d", wd, gd.at[y])
    load("q", wq, gy.at[y, :, pl.ds(0, 256)])
    load("k0", wk.at[:, pl.ds(0, 128)], gy.at[y, :, pl.ds(256, 128)])
    load("k1", wk.at[:, pl.ds(128, 128)], gz.at[z, :, pl.ds(0, 128)])
    load("v", wv, gz.at[z, :, pl.ds(128, 256)])
    load("mlp", mlp_gain, ggl.at[y])
    load("out", wo, go.at[y])
    load("up", wu, gu.at[y])
    load("down", wdn, gdn.at[y])
    load("tb", tail_b, tbb)
    load("tg", tail_g, tgg)
    for h in range(2):
        load(("tk", h), tail_k.at[:, h], kbuf.at[h])
        load(("ts", h), state.at[:, h], sbuf.at[h])
        load(("tv", h), tail_v.at[:, h], vbuf.at[h])

    loads.pop("tok").wait()

    pl.semaphore_wait(barrier, 3 * (N - 1))

    gather(TOK_A, "tp", tok_a)
    for name in ("mix", "miz", "b", "d", "q", "k0", "k1", "v", "mlp", "out"):
        loads.pop(name).wait()
    gather(G_MIX, "y", ggm)
    gather(W_B, "y", gb)
    gather(W_D, "y", gd)
    gather(G_MIZ, "z", ggz)
    gather(W_Y, "y", gy)
    gather(W_Z, "z", gz)
    gather(G_MLP, "y", ggl)
    gather(W_OUT, "y", go, (2, 6, 1, 7))
    for name in loads:
        loads[name].wait()

    bd[...] = jnp.zeros_like(bd)
    flat[...] = jnp.zeros_like(flat)
    row = iota((N * SEQ, N * SEQ), 0)
    column = iota((N * SEQ, N * SEQ), 1)
    swapped = (row // 64) * 8 + ((row // 8) % 8) * 64 + row % 8
    perm[...] = jnp.where(column == swapped, 1.0, 0.0).astype(BF)
    lens = jnp.zeros((N, T_LEN), jnp.int32)
    for i in range(N):
        lens = jnp.where(iota((N, T_LEN), 0) == i, lengths[i], lens)
    live = iota((N, T_LEN), 1) < lens
    upper = jnp.where(iota((T_LEN, T_LEN), 0) <= iota((T_LEN, T_LEN), 1), 1.0, 0.0)
    betas, gammas, totals, b3, g3, c3 = [], [], [], [], [], []
    for h in range(2):
        beta = jnp.where(live, tbb[:, h, :], 0.0)
        decay = jnp.where(live, tgg[:, h, :], 0.0)
        gamma = nn(decay, upper, HI)
        betas.append(beta)
        gammas.append(gamma)
        totals.append(jnp.sum(decay, axis=1, keepdims=True))
        b3.append(beta[:, None, :])
        g3.append(decay[:, None, :])
        c3.append(gamma[:, None, :])
    b3 = jnp.concatenate(b3, axis=0)
    g3 = jnp.concatenate(g3, axis=0)
    c3 = jnp.concatenate(c3, axis=0)
    keys = kbuf[...].reshape(2 * N, T_LEN, 128)
    gram = lax.dot_general(keys, keys, (((2,), (2,)), ((0,), (0,))), preferred_element_type=F32)
    i0 = iota((2 * N, T_LEN, T_LEN), 1)
    j0 = iota((2 * N, T_LEN, T_LEN), 2)
    diagonal = jnp.where(i0 == j0, gram, 0.0)
    inv_row = lax.rsqrt(jnp.sum(diagonal, axis=1, keepdims=True) + epsilon)
    inv_col = lax.rsqrt(jnp.sum(diagonal, axis=2, keepdims=True) + epsilon)
    gamma_col = jnp.sum(jnp.where(j0 <= i0, g3, 0.0), axis=2, keepdims=True)
    beta_col = jnp.sum(jnp.where(j0 == i0, b3, 0.0), axis=2, keepdims=True)
    below = i0 > j0
    lower = jnp.where(
        below, beta_col * jnp.exp(jnp.where(below, gamma_col - c3, 0.0)) * gram * inv_col * inv_row, 0.0
    )
    for n in range(2 * N):
        coef[n : n + 1, :] = inv_row[n]
    tri[...] = lower
    sbf[...] = sbuf[...].astype(BF)

    recv(TOK_A)
    for t in range(N):
        x32[4 * t : 4 * t + 4, :] = tok_a[t].astype(F32)
    whole = x32[...].astype(BF)
    arranged = nn(whole, perm[...])
    for t in range(N):
        xs[t] = arranged[:, 64 * t : 64 * t + 64].astype(BF)
        xzs[t] = x32[:, 64 * t : 64 * t + 64].astype(BF)
    xt[y] = xs[y]
    xzt[z] = xzs[z]
    scatter(TOK_Y, "y", xs, xt)
    scatter(TOK_Z, "z", xzs, xzt)
    gather(W_UP, "y", gu, (2, 6, 1, 7))

    for phase in (G_MIX, G_MIZ, W_B, W_D):
        recv(phase)
    for t in range(N):
        gains[0:1, 32 * t : 32 * t + 32] = ggm[t]
        gains[1:2, 32 * t : 32 * t + 32] = ggz[t]
        bd[0:2, 32 * t : 32 * t + 32] = gb[t].astype(F32)
        bd[2:4, 32 * t : 32 * t + 32] = gd[t].astype(F32)
    eye64 = jnp.where(iota((SEQ, SEQ), 0) == iota((SEQ, SEQ), 1), 1.0, 0.0).astype(BF)
    recv(TOK_Y)
    token = nt(eye64, xt[...].reshape(256, SEQ))
    xf[...] = token
    squares = jnp.sum(token * token, axis=1, keepdims=True)
    normed = (token * gains[0:1, :]).astype(BF)
    aux = nt(normed, bd[...].astype(BF))
    lane = iota((SEQ, 128), 1)
    aux = jnp.where(lane == 4, squares, aux)
    high = aux.astype(BF).astype(F32)
    aux = jnp.where(lane < 64, high, pltpu.roll(aux - high, 64, 1))
    pys[:, :, 384:512] = aux.reshape(N, N, 128).astype(BF)
    recv(W_Y)
    pys[:, :, 0:384] = nn(normed, gy[...].reshape(256, 384)).reshape(N, N, 384).astype(BF)
    pyr[z] = pys[z]
    scatter(P_Y, "z", pys, pyr)
    recv(TOK_Z)
    other = (nt(eye64, xzt[...].reshape(256, SEQ)) * gains[1:2, :]).astype(BF)
    recv(W_Z)
    pzs[...] = nn(other, gz[...].reshape(256, 384)).reshape(N, N, 384).astype(BF)
    pzr[y] = pzs[y]
    scatter(P_Z, "y", pzs, pzr)
    recv(W_OUT)
    relay(W_OUT2, "y", go)
    r0 = iota((256, 256), 0)
    r1 = iota((256, 256), 1)
    turn = jnp.where((r0 == r1) & ((r0 // 4) % N == tp), 1.0, 0.0).astype(BF)

    def part(m):
        return jnp.where((i0 // (2 * m) == j0 // (2 * m)) & (i0 // m != j0 // m), tri[...], 0.0)

    def bmm(a, b):
        return lax.dot_general(a, b, (((2,), (1,)), ((0,), (0,))), preferred_element_type=F32, precision=HI)

    inverse = jnp.where(i0 == j0, 1.0, 0.0) - part(1)
    for m in (2, 4, 8, 16, 32):
        inverse = inverse - bmm(bmm(inverse, part(m)), inverse)
    tri[...] = inverse

    recv(W_UP)
    relay(W_UP2, "y", gu)
    gather(W_DOWN, "y", gdn, (2, 6, 1, 7))
    recv(P_Y)
    raw_y = jnp.sum(pyr[...].astype(F32), axis=0)
    aux = raw_y[:, 384:512]
    aux = aux + pltpu.roll(aux, 64, 1)
    row_scale = lax.rsqrt(aux[:, 4:5] / D + epsilon)
    raw_y = raw_y * row_scale
    recv(P_Z)
    raw_z = jnp.sum(pzr[...].astype(F32), axis=0) * row_scale
    results = []
    for h in range(2):
        query = unit(silu(raw_y[:, 128 * h : 128 * h + 128]))
        key = unit(silu(raw_y[:, 256:384] if h == 0 else raw_z[:, 0:128]))
        value = silu(raw_z[:, 128 + 128 * h : 256 + 128 * h])
        new_beta = 1.0 / (1.0 + jnp.exp(-(aux[:, h : h + 1] * row_scale)))
        pre = aux[:, 2 + h : 3 + h] * row_scale
        soft = jnp.maximum(pre, 0.0) + jnp.log(1.0 + jnp.exp(-jnp.abs(pre)))
        new_decay = -rate[h] * soft
        weight = new_beta * jnp.sum(key * query, axis=1, keepdims=True)
        test = query - weight * key
        inv = coef[N * h : N * h + N, :]
        a = rows_by(test, kbuf[h], 2) * jnp.exp(totals[h] - gammas[h]) * inv
        lhs = jnp.broadcast_to(a[None], (N, N, T_LEN))
        solved = own_row(bmm(lhs, tri[N * h : N * h + N])) * betas[h]
        from_values = rows_by(solved, vbuf[h], 1)
        moved = jnp.exp(totals[h]) * test - rows_by(solved * jnp.exp(gammas[h]) * inv, kbuf[h], 1)
        readout = rows_by(moved, sbf[h], 1) + from_values
        results.append(jnp.exp(new_decay) * readout + weight * value)
    heads[z] = jnp.concatenate(results, axis=1).astype(BF)
    gather(HEADS, "z", heads)

    recv(W_OUT2)
    recv(G_MLP)
    for t in range(N):
        gains[2:3, 32 * t : 32 * t + 32] = ggl[t]
    recv(HEADS)
    gathered = heads[...].astype(F32).reshape(SEQ, 256).astype(BF)
    att[tp] = nt(gathered, go[...].reshape(256, 256)).astype(BF)
    gather(ATT, "tp", att)
    recv(W_UP2)
    recv(ATT)
    mixed[...] = (xf[...] + jnp.sum(att[...].astype(F32), axis=0)).astype(BF)
    mixer = mixed[...].astype(F32)
    normed = (mixer * gains[2:3, :]).astype(BF)
    ums[:, :, 0:1024] = nn(normed, gu[...].reshape(256, 1024)).reshape(N, N, 1024).astype(BF)
    squares = jnp.sum(mixer * mixer, axis=1, keepdims=True)
    high = squares.astype(BF).astype(F32)
    ums[:, :, 1024:1152] = jnp.where(lane < 64, high, squares - high).reshape(N, N, 128).astype(BF)
    umr[z] = ums[z]
    scatter(U_MAIN, "z", ums, umr)
    recv(W_DOWN)
    relay(W_DOWN2, "y", gdn)
    mixt[...] = nt(turn, mixed[...])
    recv(U_MAIN)
    raw = jnp.sum(umr[...].astype(F32), axis=0)
    row_scale = lax.rsqrt((raw[:, 1024:1025] + raw[:, 1088:1089]) / D + epsilon)
    raw = jnp.maximum(raw[:, 0:1024] * row_scale, 0.0)
    hid[z] = (raw * raw).astype(BF)
    gather(HID, "z", hid)
    recv(W_DOWN2)
    recv(HID)
    hidden = hid[...].astype(F32).reshape(SEQ, 1024).astype(BF)
    down_t[...] = nt(gdn[...].reshape(256, 1024), hidden) + mixt[...]
    for t in range(N * N):
        dns[t] = down_t[4 * t : 4 * t + 4, :].astype(BF)
    for a in (4, 3, 5, 2, 6, 1, 7, 0):
        for b in (4, 3, 5, 2, 6, 1, 7, 0):
            if a or b:
                to_y, to_tp = (y + a) % N, (tp + b) % N
                pltpu.make_async_remote_copy(
                    src_ref=dns.at[to_y * N + to_tp],
                    dst_ref=dnr.at[y * N + tp],
                    send_sem=send_sem.at[DOWN],
                    recv_sem=recv_sem.at[DOWN],
                    device_id=(z * N + to_y, to_tp),
                    device_id_type=MESH,
                ).start()
    dnr[y * N + tp] = dns[y * N + tp]
    for phase, buf, count in started:
        part_of = buf.at[pl.ds(0, count)]
        pltpu.make_async_copy(part_of, part_of, send_sem.at[phase]).wait()
    others = dnr.at[pl.ds(0, N * N - 1)]
    pltpu.make_async_copy(others, others, recv_sem.at[DOWN]).wait()
    for t in range(N):
        block = jnp.sum(dnr[N * t : N * t + N].astype(F32), axis=0)
        flat[0:4, 64 * t : 64 * t + 64] = block
    out[...] = nn(flat[...].astype(BF), perm[...])[0:4, :].astype(BF)
    pltpu.make_async_copy(others, others, send_sem.at[DOWN]).wait()


def local(
    tokens, mix_gain, query_weight, key_weight, value_weight, beta_weight, decay_weight, decay_rate, prior_state,
    tail_keys, tail_values, tail_beta, tail_decay, lengths, out_weight, mlp_gain, up_weight, down_weight,
):
    vmem = pl.BlockSpec(memory_space=pltpu.VMEM)
    smem = pl.BlockSpec(memory_space=pltpu.SMEM)
    hbm = pl.BlockSpec(memory_space=pl.ANY)
    specs = [hbm] * 7 + [smem] + [hbm] * 5 + [smem] + [hbm] * 4

    def v(*shape, dtype=BF):
        return pltpu.VMEM(shape, dtype)

    def f(*shape):
        return v(*shape, dtype=F32)

    result = pl.pallas_call(
        kernel,
        out_shape=jax.ShapeDtypeStruct((4, 512), BF),
        in_specs=specs,
        out_specs=vmem,
        scratch_shapes=[
            v(8, 4, 512), f(32, 512), v(512, 512), v(8, 32, 64), v(8, 32, 64), v(8, 32, 64), v(8, 32, 64), f(64, 256),
            v(8, 32, 384), v(8, 32, 384), v(8, 2, 32), v(8, 2, 32), f(8, 1, 32), f(8, 1, 32), f(8, 1, 32),
            v(8, 32, 256), v(8, 32, 1024), v(8, 32, 1024), f(128, 256), f(8, 256),
            v(2, 8, 64, 128), v(2, 8, 64, 128), f(2, 8, 128, 128), v(2, 8, 128, 128), f(8, 2, 64), f(8, 2, 64),
            f(16, 64, 64), f(16, 64),
            v(8, 8, 512), v(8, 8, 512), v(8, 8, 384), v(8, 8, 384),
            v(8, 8, 256), v(8, 64, 256), v(64, 256), f(256, 64),
            v(8, 8, 1152), v(8, 8, 1152),
            v(8, 8, 1024), f(256, 64), v(64, 4, 64), v(64, 4, 64), f(8, 512),
            pltpu.SemaphoreType.DMA((23,)), pltpu.SemaphoreType.DMA((23,)), pltpu.SemaphoreType.DMA((21,)),
        ],
        compiler_params=pltpu.CompilerParams(collective_id=0, has_side_effects=True),
    )(
        tokens.T, mix_gain.reshape(1, -1), query_weight, key_weight, value_weight, beta_weight.T, decay_weight.T,
        decay_rate, prior_state, tail_keys, tail_values, tail_beta, tail_decay, lengths, out_weight.T,
        mlp_gain.reshape(1, -1), up_weight, down_weight.T,
    )
    return result.T


def solution(mesh):
    kt = ("kv", "tp")
    return jax.shard_map(
        local,
        mesh=mesh,
        in_specs=(
            P(None, kt), P("kv"), P("kv", "tp"), P("kv", "tp"), P("kv", "tp"), P("kv", "tp"), P("kv", "tp"), P("tp"),
            P("kv", "tp", None, None), P("kv", "tp", None, None), P("kv", "tp", None, None),
            P("kv", "tp", None), P("kv", "tp", None), P("kv"), P("tp", "kv"), P("kv"), P("kv", "tp"), P("tp", "kv"),
        ),
        out_specs=P(None, kt),
        check_vma=False,
    )
```

```python
import jax
import jax.numpy as jnp
from jax import lax
from jax.experimental import pallas as pl
from jax.experimental.pallas import tpu as pltpu
from jax.sharding import PartitionSpec as P

D = 2048
N = 8
SEQ = 64
T_LEN = 64
epsilon = 1e-06
BF = jnp.bfloat16
F32 = jnp.float32
HI = lax.Precision.HIGHEST
MESH = pl.DeviceIdType.MESH

(TOK_A, TOK_Y, TOK_Z, W_Y, W_Z, W_B, W_D, G_MIX, G_MIZ, G_MLP, W_OUT, W_OUT2, W_UP, W_UP2, W_DOWN, W_DOWN2,
 P_Y, P_Z, HEADS, ATT, U_MAIN, HID, DOWN) = range(23)
FAR_FIRST = (4, 3, 5, 2, 6, 1, 7)


def nt(a, b, precision=None):
    return lax.dot_general(a, b, (((1,), (1,)), ((), ())), preferred_element_type=F32, precision=precision)


def nn(a, b, precision=None):
    return lax.dot_general(a, b, (((1,), (0,)), ((), ())), preferred_element_type=F32, precision=precision)


def iota(shape, dim):
    return lax.broadcasted_iota(jnp.int32, shape, dim)


def split_rows(x):
    high = x.astype(BF)
    low = (x - high.astype(F32)).astype(BF)
    return jnp.concatenate([high.astype(F32), low.astype(F32)], axis=0).astype(BF)


def own_row(r):
    return jnp.sum(jnp.where(iota(r.shape, 0) == iota(r.shape, 1), r, 0.0), axis=0)


def rows_by(x, mats, contract):
    both = split_rows(x)
    lhs = jnp.broadcast_to(both[None], (N, *both.shape))
    r = lax.dot_general(lhs, mats, (((2,), (contract,)), ((0,), (0,))), preferred_element_type=F32)
    return own_row(r[:, :N] + r[:, N:])


def unit(x):
    return x * lax.rsqrt(jnp.sum(x * x, axis=-1, keepdims=True) + epsilon)


def silu(x):
    return x * (1.0 / (1.0 + jnp.exp(-x)))


def kernel(
    tok, mix_gain, wq, wk, wv, wb, wd, rate_in, state, tail_k, tail_v, tail_b, tail_g, lengths_in, wo, mlp_gain, wu, wdn,
    out,
    tok_a, x32, perm, xs, xt, xzs, xzt, xf, gy, gz, gb, gd, ggm, ggz, ggl, go, gu, gdn, bd, gains,
    kbuf, vbuf, sbuf, sbf, tbb, tgg, tri, coef, pys, pyr, pzs, pzr, heads, att, mixed, mixt,
    ums, umr, hid, down_t, dns, dnr, flat, lengths, rate, send_sem, recv_sem, local_sem,
):
    kv = lax.axis_index("kv")
    tp = lax.axis_index("tp")
    z = kv // N
    y = kv % N

    def peer(axis, r):
        if axis == "z":
            return (((z + r) % N) * N + y, tp)
        if axis == "y":
            return (z * N + (y + r) % N, tp)
        return (kv, (tp + r) % N)

    me = {"z": z, "y": y, "tp": tp}
    started = []

    def copy(phase, axis, src, dst, r):
        pltpu.make_async_remote_copy(
            src_ref=src,
            dst_ref=dst,
            send_sem=send_sem.at[phase],
            recv_sem=recv_sem.at[phase],
            device_id=peer(axis, r),
            device_id_type=MESH,
        ).start()

    def gather(phase, axis, buf, steps=FAR_FIRST):
        started.append((phase, buf, len(steps)))
        for r in steps:
            copy(phase, axis, buf.at[me[axis]], buf.at[me[axis]], r)

    def scatter(phase, axis, src, dst):
        started.append((phase, dst, N - 1))
        for r in FAR_FIRST:
            copy(phase, axis, src.at[(me[axis] + r) % N], dst.at[me[axis]], r)

    def relay(phase, axis, buf):
        started.append((phase, buf, 3))
        behind, ahead = (me[axis] + N - 2) % N, (me[axis] + 2) % N
        copy(phase, axis, buf.at[behind], buf.at[behind], 2)
        copy(phase, axis, buf.at[behind], buf.at[behind], 1)
        copy(phase, axis, buf.at[ahead], buf.at[ahead], 7)

    def recv(phase):
        for p, buf, count in started:
            if p == phase:
                part = buf.at[pl.ds(0, count)]
                pltpu.make_async_copy(part, part, recv_sem.at[phase]).wait()

    barrier = pltpu.get_barrier_semaphore()
    for r in FAR_FIRST:
        for axis in ("z", "y", "tp"):
            pl.semaphore_signal(barrier, inc=1, device_id=peer(axis, r), device_id_type=MESH)

    loads = {}

    def load(name, src, dst):
        c = pltpu.make_async_copy(src, dst, local_sem.at[len(loads)])
        c.start()
        loads[name] = c

    load("tok", tok, tok_a.at[tp])
    load("mix", mix_gain, ggm.at[y])
    load("miz", mix_gain, ggz.at[z])
    load("b", wb, gb.at[y])
    load("d", wd, gd.at[y])
    load("q", wq, gy.at[y, :, pl.ds(0, 256)])
    load("k0", wk.at[:, pl.ds(0, 128)], gy.at[y, :, pl.ds(256, 128)])
    load("k1", wk.at[:, pl.ds(128, 128)], gz.at[z, :, pl.ds(0, 128)])
    load("v", wv, gz.at[z, :, pl.ds(128, 256)])
    load("mlp", mlp_gain, ggl.at[y])
    load("out", wo, go.at[y])
    load("up", wu, gu.at[y])
    load("down", wdn, gdn.at[y])
    load("lengths", lengths_in, lengths)
    load("rate", rate_in, rate)
    load("tb", tail_b, tbb)
    load("tg", tail_g, tgg)
    for h in range(2):
        load(("tk", h), tail_k.at[:, h], kbuf.at[h])
        load(("ts", h), state.at[:, h], sbuf.at[h])
        load(("tv", h), tail_v.at[:, h], vbuf.at[h])

    loads.pop("tok").wait()

    pl.semaphore_wait(barrier, 3 * (N - 1))

    gather(TOK_A, "tp", tok_a)
    for name in ("mix", "miz", "b", "d", "q", "k0", "k1", "v", "mlp", "out"):
        loads.pop(name).wait()
    gather(G_MIX, "y", ggm)
    gather(W_B, "y", gb)
    gather(W_D, "y", gd)
    gather(G_MIZ, "z", ggz)
    gather(W_Y, "y", gy)
    gather(W_Z, "z", gz)
    gather(G_MLP, "y", ggl)
    gather(W_OUT, "y", go, (2, 6, 1, 7))
    for name in loads:
        loads[name].wait()

    bd[...] = jnp.zeros_like(bd)
    flat[...] = jnp.zeros_like(flat)
    row = iota((N * SEQ, N * SEQ), 0)
    column = iota((N * SEQ, N * SEQ), 1)
    swapped = (row // 64) * 8 + ((row // 8) % 8) * 64 + row % 8
    perm[...] = jnp.where(column == swapped, 1.0, 0.0).astype(BF)
    lens = jnp.zeros((N, T_LEN), jnp.int32)
    for i in range(N):
        lens = jnp.where(iota((N, T_LEN), 0) == i, lengths[i], lens)
    live = iota((N, T_LEN), 1) < lens
    upper = jnp.where(iota((T_LEN, T_LEN), 0) <= iota((T_LEN, T_LEN), 1), 1.0, 0.0)
    betas, gammas, totals, b3, g3, c3 = [], [], [], [], [], []
    for h in range(2):
        beta = jnp.where(live, tbb[:, h, :], 0.0)
        decay = jnp.where(live, tgg[:, h, :], 0.0)
        gamma = nn(decay, upper, HI)
        betas.append(beta)
        gammas.append(gamma)
        totals.append(jnp.sum(decay, axis=1, keepdims=True))
        b3.append(beta[:, None, :])
        g3.append(decay[:, None, :])
        c3.append(gamma[:, None, :])
    b3 = jnp.concatenate(b3, axis=0)
    g3 = jnp.concatenate(g3, axis=0)
    c3 = jnp.concatenate(c3, axis=0)
    keys = kbuf[...].reshape(2 * N, T_LEN, 128)
    gram = lax.dot_general(keys, keys, (((2,), (2,)), ((0,), (0,))), preferred_element_type=F32)
    i0 = iota((2 * N, T_LEN, T_LEN), 1)
    j0 = iota((2 * N, T_LEN, T_LEN), 2)
    diagonal = jnp.where(i0 == j0, gram, 0.0)
    inv_row = lax.rsqrt(jnp.sum(diagonal, axis=1, keepdims=True) + epsilon)
    inv_col = lax.rsqrt(jnp.sum(diagonal, axis=2, keepdims=True) + epsilon)
    gamma_col = jnp.sum(jnp.where(j0 <= i0, g3, 0.0), axis=2, keepdims=True)
    beta_col = jnp.sum(jnp.where(j0 == i0, b3, 0.0), axis=2, keepdims=True)
    below = i0 > j0
    lower = jnp.where(
        below, beta_col * jnp.exp(jnp.where(below, gamma_col - c3, 0.0)) * gram * inv_col * inv_row, 0.0
    )
    for n in range(2 * N):
        coef[n : n + 1, :] = inv_row[n]
    tri[...] = lower
    sbf[...] = sbuf[...].astype(BF)

    recv(TOK_A)
    for t in range(N):
        x32[4 * t : 4 * t + 4, :] = tok_a[t].astype(F32)
    whole = x32[...].astype(BF)
    arranged = nn(whole, perm[...])
    for t in range(N):
        xs[t] = arranged[:, 64 * t : 64 * t + 64].astype(BF)
        xzs[t] = x32[:, 64 * t : 64 * t + 64].astype(BF)
    xt[y] = xs[y]
    xzt[z] = xzs[z]
    scatter(TOK_Y, "y", xs, xt)
    scatter(TOK_Z, "z", xzs, xzt)
    gather(W_UP, "y", gu, (2, 6, 1, 7))

    for phase in (G_MIX, G_MIZ, W_B, W_D):
        recv(phase)
    for t in range(N):
        gains[0:1, 32 * t : 32 * t + 32] = ggm[t]
        gains[1:2, 32 * t : 32 * t + 32] = ggz[t]
        bd[0:2, 32 * t : 32 * t + 32] = gb[t].astype(F32)
        bd[2:4, 32 * t : 32 * t + 32] = gd[t].astype(F32)
    eye64 = jnp.where(iota((SEQ, SEQ), 0) == iota((SEQ, SEQ), 1), 1.0, 0.0).astype(BF)
    recv(TOK_Y)
    token = nt(eye64, xt[...].reshape(256, SEQ))
    xf[...] = token
    squares = jnp.sum(token * token, axis=1, keepdims=True)
    normed = (token * gains[0:1, :]).astype(BF)
    aux = nt(normed, bd[...].astype(BF))
    lane = iota((SEQ, 128), 1)
    aux = jnp.where(lane == 4, squares, aux)
    high = aux.astype(BF).astype(F32)
    aux = jnp.where(lane < 64, high, pltpu.roll(aux - high, 64, 1))
    pys[:, :, 384:512] = aux.reshape(N, N, 128).astype(BF)
    recv(W_Y)
    pys[:, :, 0:384] = nn(normed, gy[...].reshape(256, 384)).reshape(N, N, 384).astype(BF)
    pyr[z] = pys[z]
    scatter(P_Y, "z", pys, pyr)
    recv(TOK_Z)
    other = (nt(eye64, xzt[...].reshape(256, SEQ)) * gains[1:2, :]).astype(BF)
    recv(W_Z)
    pzs[...] = nn(other, gz[...].reshape(256, 384)).reshape(N, N, 384).astype(BF)
    pzr[y] = pzs[y]
    scatter(P_Z, "y", pzs, pzr)
    recv(W_OUT)
    relay(W_OUT2, "y", go)
    r0 = iota((256, 256), 0)
    r1 = iota((256, 256), 1)
    turn = jnp.where((r0 == r1) & ((r0 // 4) % N == tp), 1.0, 0.0).astype(BF)

    def part(m):
        return jnp.where((i0 // (2 * m) == j0 // (2 * m)) & (i0 // m != j0 // m), tri[...], 0.0)

    def bmm(a, b):
        return lax.dot_general(a, b, (((2,), (1,)), ((0,), (0,))), preferred_element_type=F32, precision=HI)

    inverse = jnp.where(i0 == j0, 1.0, 0.0) - part(1)
    for m in (2, 4, 8, 16, 32):
        inverse = inverse - bmm(bmm(inverse, part(m)), inverse)
    tri[...] = inverse

    recv(W_UP)
    relay(W_UP2, "y", gu)
    gather(W_DOWN, "y", gdn, (2, 6, 1, 7))
    recv(P_Y)
    raw_y = jnp.sum(pyr[...].astype(F32), axis=0)
    aux = raw_y[:, 384:512]
    aux = aux + pltpu.roll(aux, 64, 1)
    row_scale = lax.rsqrt(aux[:, 4:5] / D + epsilon)
    raw_y = raw_y * row_scale
    recv(P_Z)
    raw_z = jnp.sum(pzr[...].astype(F32), axis=0) * row_scale
    results = []
    for h in range(2):
        query = unit(silu(raw_y[:, 128 * h : 128 * h + 128]))
        key = unit(silu(raw_y[:, 256:384] if h == 0 else raw_z[:, 0:128]))
        value = silu(raw_z[:, 128 + 128 * h : 256 + 128 * h])
        new_beta = 1.0 / (1.0 + jnp.exp(-(aux[:, h : h + 1] * row_scale)))
        pre = aux[:, 2 + h : 3 + h] * row_scale
        soft = jnp.maximum(pre, 0.0) + jnp.log(1.0 + jnp.exp(-jnp.abs(pre)))
        new_decay = -rate[h] * soft
        weight = new_beta * jnp.sum(key * query, axis=1, keepdims=True)
        test = query - weight * key
        inv = coef[N * h : N * h + N, :]
        a = rows_by(test, kbuf[h], 2) * jnp.exp(totals[h] - gammas[h]) * inv
        lhs = jnp.broadcast_to(a[None], (N, N, T_LEN))
        solved = own_row(bmm(lhs, tri[N * h : N * h + N])) * betas[h]
        from_values = rows_by(solved, vbuf[h], 1)
        moved = jnp.exp(totals[h]) * test - rows_by(solved * jnp.exp(gammas[h]) * inv, kbuf[h], 1)
        readout = rows_by(moved, sbf[h], 1) + from_values
        results.append(jnp.exp(new_decay) * readout + weight * value)
    heads[z] = jnp.concatenate(results, axis=1).astype(BF)
    gather(HEADS, "z", heads)

    recv(W_OUT2)
    recv(G_MLP)
    for t in range(N):
        gains[2:3, 32 * t : 32 * t + 32] = ggl[t]
    recv(HEADS)
    gathered = heads[...].astype(F32).reshape(SEQ, 256).astype(BF)
    att[tp] = nt(gathered, go[...].reshape(256, 256)).astype(BF)
    gather(ATT, "tp", att)
    recv(W_UP2)
    recv(ATT)
    mixed[...] = (xf[...] + jnp.sum(att[...].astype(F32), axis=0)).astype(BF)
    mixer = mixed[...].astype(F32)
    normed = (mixer * gains[2:3, :]).astype(BF)
    ums[:, :, 0:1024] = nn(normed, gu[...].reshape(256, 1024)).reshape(N, N, 1024).astype(BF)
    squares = jnp.sum(mixer * mixer, axis=1, keepdims=True)
    high = squares.astype(BF).astype(F32)
    ums[:, :, 1024:1152] = jnp.where(lane < 64, high, squares - high).reshape(N, N, 128).astype(BF)
    umr[z] = ums[z]
    scatter(U_MAIN, "z", ums, umr)
    recv(W_DOWN)
    relay(W_DOWN2, "y", gdn)
    mixt[...] = nt(turn, mixed[...])
    recv(U_MAIN)
    raw = jnp.sum(umr[...].astype(F32), axis=0)
    row_scale = lax.rsqrt((raw[:, 1024:1025] + raw[:, 1088:1089]) / D + epsilon)
    raw = jnp.maximum(raw[:, 0:1024] * row_scale, 0.0)
    hid[z] = (raw * raw).astype(BF)
    gather(HID, "z", hid)
    recv(W_DOWN2)
    recv(HID)
    hidden = hid[...].astype(F32).reshape(SEQ, 1024).astype(BF)
    down_t[...] = nt(gdn[...].reshape(256, 1024), hidden) + mixt[...]
    for t in range(N * N):
        dns[t] = down_t[4 * t : 4 * t + 4, :].astype(BF)
    for a in (4, 3, 5, 2, 6, 1, 7, 0):
        for b in (4, 3, 5, 2, 6, 1, 7, 0):
            if a or b:
                to_y, to_tp = (y + a) % N, (tp + b) % N
                pltpu.make_async_remote_copy(
                    src_ref=dns.at[to_y * N + to_tp],
                    dst_ref=dnr.at[y * N + tp],
                    send_sem=send_sem.at[DOWN],
                    recv_sem=recv_sem.at[DOWN],
                    device_id=(z * N + to_y, to_tp),
                    device_id_type=MESH,
                ).start()
    dnr[y * N + tp] = dns[y * N + tp]
    for phase, buf, count in started:
        part_of = buf.at[pl.ds(0, count)]
        pltpu.make_async_copy(part_of, part_of, send_sem.at[phase]).wait()
    others = dnr.at[pl.ds(0, N * N - 1)]
    pltpu.make_async_copy(others, others, recv_sem.at[DOWN]).wait()
    for t in range(N):
        block = jnp.sum(dnr[N * t : N * t + N].astype(F32), axis=0)
        flat[0:4, 64 * t : 64 * t + 64] = block
    out[...] = nn(flat[...].astype(BF), perm[...])[0:4, :].astype(BF)
    pltpu.make_async_copy(others, others, send_sem.at[DOWN]).wait()


def local(
    tokens, mix_gain, query_weight, key_weight, value_weight, beta_weight, decay_weight, decay_rate, prior_state,
    tail_keys, tail_values, tail_beta, tail_decay, lengths, out_weight, mlp_gain, up_weight, down_weight,
):
    vmem = pl.BlockSpec(memory_space=pltpu.VMEM)
    hbm = pl.BlockSpec(memory_space=pl.ANY)
    specs = [hbm] * 18

    def v(*shape, dtype=BF):
        return pltpu.VMEM(shape, dtype)

    def f(*shape):
        return v(*shape, dtype=F32)

    result = pl.pallas_call(
        kernel,
        out_shape=jax.ShapeDtypeStruct((4, 512), BF),
        in_specs=specs,
        out_specs=vmem,
        scratch_shapes=[
            v(8, 4, 512), f(32, 512), v(512, 512), v(8, 32, 64), v(8, 32, 64), v(8, 32, 64), v(8, 32, 64), f(64, 256),
            v(8, 32, 384), v(8, 32, 384), v(8, 2, 32), v(8, 2, 32), f(8, 1, 32), f(8, 1, 32), f(8, 1, 32),
            v(8, 32, 256), v(8, 32, 1024), v(8, 32, 1024), f(128, 256), f(8, 256),
            v(2, 8, 64, 128), v(2, 8, 64, 128), f(2, 8, 128, 128), v(2, 8, 128, 128), f(8, 2, 64), f(8, 2, 64),
            f(16, 64, 64), f(16, 64),
            v(8, 8, 512), v(8, 8, 512), v(8, 8, 384), v(8, 8, 384),
            v(8, 8, 256), v(8, 64, 256), v(64, 256), f(256, 64),
            v(8, 8, 1152), v(8, 8, 1152),
            v(8, 8, 1024), f(256, 64), v(64, 4, 64), v(64, 4, 64), f(8, 512),
            pltpu.SMEM((8,), jnp.int32), pltpu.SMEM((2,), F32),
            pltpu.SemaphoreType.DMA((23,)), pltpu.SemaphoreType.DMA((23,)), pltpu.SemaphoreType.DMA((23,)),
        ],
        compiler_params=pltpu.CompilerParams(collective_id=0, has_side_effects=True),
    )(
        tokens.T, mix_gain.reshape(1, -1), query_weight, key_weight, value_weight, beta_weight.T, decay_weight.T,
        decay_rate, prior_state, tail_keys, tail_values, tail_beta, tail_decay, lengths, out_weight.T,
        mlp_gain.reshape(1, -1), up_weight, down_weight.T,
    )
    return result.T


def solution(mesh):
    kt = ("kv", "tp")
    return jax.shard_map(
        local,
        mesh=mesh,
        in_specs=(
            P(None, kt), P("kv"), P("kv", "tp"), P("kv", "tp"), P("kv", "tp"), P("kv", "tp"), P("kv", "tp"), P("tp"),
            P("kv", "tp", None, None), P("kv", "tp", None, None), P("kv", "tp", None, None),
            P("kv", "tp", None), P("kv", "tp", None), P("kv"), P("tp", "kv"), P("kv"), P("kv", "tp"), P("tp", "kv"),
        ),
        out_specs=P(None, kt),
        check_vma=False,
    )
```

```python
import jax
import jax.numpy as jnp
from jax import lax
from jax.experimental import pallas as pl
from jax.experimental.pallas import tpu as pltpu
from jax.sharding import PartitionSpec as P

D = 2048
N = 8
SEQ = 64
T_LEN = 64
epsilon = 1e-06
BF = jnp.bfloat16
F32 = jnp.float32
HI = lax.Precision.HIGHEST
MESH = pl.DeviceIdType.MESH

(TOK_A, TOK_Y, TOK_Z, W_Y, W_Z, W_B, W_D, G_MIX, G_MIZ, G_MLP, W_OUT, W_OUT2, W_UP, W_UP2, W_DOWN, W_DOWN2,
 P_Y, P_Z, HEADS, ATT, U_MAIN, HID, DOWN) = range(23)
FAR_FIRST = (4, 3, 5, 2, 6, 1, 7)


def nt(a, b, precision=None):
    return lax.dot_general(a, b, (((1,), (1,)), ((), ())), preferred_element_type=F32, precision=precision)


def nn(a, b, precision=None):
    return lax.dot_general(a, b, (((1,), (0,)), ((), ())), preferred_element_type=F32, precision=precision)


def iota(shape, dim):
    return lax.broadcasted_iota(jnp.int32, shape, dim)


def split_rows(x):
    high = x.astype(BF)
    low = (x - high.astype(F32)).astype(BF)
    return jnp.concatenate([high.astype(F32), low.astype(F32)], axis=0).astype(BF)


def own_row(r):
    return jnp.sum(jnp.where(iota(r.shape, 0) == iota(r.shape, 1), r, 0.0), axis=0)


def rows_by(x, mats, contract):
    both = split_rows(x)
    lhs = jnp.broadcast_to(both[None], (N, *both.shape))
    r = lax.dot_general(lhs, mats, (((2,), (contract,)), ((0,), (0,))), preferred_element_type=F32)
    return own_row(r[:, :N] + r[:, N:])


def unit(x):
    return x * lax.rsqrt(jnp.sum(x * x, axis=-1, keepdims=True) + epsilon)


def silu(x):
    return x * (1.0 / (1.0 + jnp.exp(-x)))


def kernel(
    tok, mix_gain, wq, wk, wv, wb, wd, rate_in, state, tail_k, tail_v, tail_b, tail_g, lengths_in, wo, mlp_gain, wu, wdn,
    out,
    tok_a, x32, perm, xs, xt, xzs, xzt, xf, gy, gz, gb, gd, ggm, ggz, ggl, go, gu, gdn, bd, gains,
    kbuf, vbuf, sbuf, sbf, tbb, tgg, tri, coef, pys, pyr, pzs, pzr, heads, att, mixed, mixt,
    ums, umr, hid, down_t, dns, dnr, flat, lengths, rate, send_sem, recv_sem, local_sem,
):
    kv = lax.axis_index("kv")
    tp = lax.axis_index("tp")
    z = kv // N
    y = kv % N

    def peer(axis, r):
        if axis == "z":
            return (((z + r) % N) * N + y, tp)
        if axis == "y":
            return (z * N + (y + r) % N, tp)
        return (kv, (tp + r) % N)

    me = {"z": z, "y": y, "tp": tp}
    started = []

    def copy(phase, axis, src, dst, r):
        pltpu.make_async_remote_copy(
            src_ref=src,
            dst_ref=dst,
            send_sem=send_sem.at[phase],
            recv_sem=recv_sem.at[phase],
            device_id=peer(axis, r),
            device_id_type=MESH,
        ).start()

    def gather(phase, axis, buf, steps=FAR_FIRST):
        started.append((phase, buf, len(steps)))
        for r in steps:
            copy(phase, axis, buf.at[me[axis]], buf.at[me[axis]], r)

    def scatter(phase, axis, src, dst):
        started.append((phase, dst, N - 1))
        for r in FAR_FIRST:
            copy(phase, axis, src.at[(me[axis] + r) % N], dst.at[me[axis]], r)

    def relay(phase, axis, buf):
        started.append((phase, buf, 3))
        behind, ahead = (me[axis] + N - 2) % N, (me[axis] + 2) % N
        copy(phase, axis, buf.at[behind], buf.at[behind], 2)
        copy(phase, axis, buf.at[behind], buf.at[behind], 1)
        copy(phase, axis, buf.at[ahead], buf.at[ahead], 7)

    def recv(phase):
        for p, buf, count in started:
            if p == phase:
                part = buf.at[pl.ds(0, count)]
                pltpu.make_async_copy(part, part, recv_sem.at[phase]).wait()

    barrier = pltpu.get_barrier_semaphore()
    for r in FAR_FIRST:
        for axis in ("z", "y", "tp"):
            pl.semaphore_signal(barrier, inc=1, device_id=peer(axis, r), device_id_type=MESH)

    loads = {}

    def load(name, src, dst):
        c = pltpu.make_async_copy(src, dst, local_sem.at[len(loads)])
        c.start()
        loads[name] = c

    load("tok", tok, tok_a.at[tp])
    load("mix", mix_gain, ggm.at[y])
    load("miz", mix_gain, ggz.at[z])
    load("b", wb, gb.at[y])
    load("d", wd, gd.at[y])
    load("q", wq, gy.at[y, :, pl.ds(0, 256)])
    load("k0", wk.at[:, pl.ds(0, 128)], gy.at[y, :, pl.ds(256, 128)])
    load("k1", wk.at[:, pl.ds(128, 128)], gz.at[z, :, pl.ds(0, 128)])
    load("v", wv, gz.at[z, :, pl.ds(128, 256)])
    load("mlp", mlp_gain, ggl.at[y])
    load("out", wo, go.at[y])
    load("up", wu, gu.at[y])
    load("down", wdn, gdn.at[y])
    load("lengths", lengths_in, lengths)
    load("rate", rate_in, rate)
    load("tb", tail_b, tbb)
    load("tg", tail_g, tgg)
    for h in range(2):
        load(("tk", h), tail_k.at[:, h], kbuf.at[h])
        load(("ts", h), state.at[:, h], sbuf.at[h])
        load(("tv", h), tail_v.at[:, h], vbuf.at[h])

    loads.pop("tok").wait()

    pl.semaphore_wait(barrier, 3 * (N - 1))

    gather(TOK_A, "tp", tok_a)
    for name in ("mix", "miz", "b", "d", "q", "k0", "k1", "v", "mlp", "out"):
        loads.pop(name).wait()
    gather(G_MIX, "y", ggm)
    gather(W_B, "y", gb)
    gather(W_D, "y", gd)
    gather(G_MIZ, "z", ggz)
    gather(W_Y, "y", gy)
    gather(W_Z, "z", gz)
    gather(G_MLP, "y", ggl)
    gather(W_OUT, "y", go, (2, 6, 1, 7))
    for name in loads:
        loads[name].wait()

    bd[...] = jnp.zeros_like(bd)
    flat[...] = jnp.zeros_like(flat)
    row = iota((N * SEQ, N * SEQ), 0)
    column = iota((N * SEQ, N * SEQ), 1)
    swapped = (row // 64) * 8 + ((row // 8) % 8) * 64 + row % 8
    perm[...] = jnp.where(column == swapped, 1.0, 0.0).astype(BF)
    lens = jnp.zeros((N, T_LEN), jnp.int32)
    for i in range(N):
        lens = jnp.where(iota((N, T_LEN), 0) == i, lengths[i], lens)
    live = iota((N, T_LEN), 1) < lens
    upper = jnp.where(iota((T_LEN, T_LEN), 0) <= iota((T_LEN, T_LEN), 1), 1.0, 0.0)
    betas, gammas, totals, b3, g3, c3 = [], [], [], [], [], []
    for h in range(2):
        beta = jnp.where(live, tbb[:, h, :], 0.0)
        decay = jnp.where(live, tgg[:, h, :], 0.0)
        gamma = nn(decay, upper, HI)
        betas.append(beta)
        gammas.append(gamma)
        totals.append(jnp.sum(decay, axis=1, keepdims=True))
        b3.append(beta[:, None, :])
        g3.append(decay[:, None, :])
        c3.append(gamma[:, None, :])
    b3 = jnp.concatenate(b3, axis=0)
    g3 = jnp.concatenate(g3, axis=0)
    c3 = jnp.concatenate(c3, axis=0)
    keys = kbuf[...].reshape(2 * N, T_LEN, 128)
    gram = lax.dot_general(keys, keys, (((2,), (2,)), ((0,), (0,))), preferred_element_type=F32)
    i0 = iota((2 * N, T_LEN, T_LEN), 1)
    j0 = iota((2 * N, T_LEN, T_LEN), 2)
    diagonal = jnp.where(i0 == j0, gram, 0.0)
    inv_row = lax.rsqrt(jnp.sum(diagonal, axis=1, keepdims=True) + epsilon)
    inv_col = lax.rsqrt(jnp.sum(diagonal, axis=2, keepdims=True) + epsilon)
    gamma_col = jnp.sum(jnp.where(j0 <= i0, g3, 0.0), axis=2, keepdims=True)
    beta_col = jnp.sum(jnp.where(j0 == i0, b3, 0.0), axis=2, keepdims=True)
    below = i0 > j0
    lower = jnp.where(
        below, beta_col * jnp.exp(jnp.where(below, gamma_col - c3, 0.0)) * gram * inv_col * inv_row, 0.0
    )
    for n in range(2 * N):
        coef[n : n + 1, :] = inv_row[n]
    tri[...] = lower
    sbf[...] = sbuf[...].astype(BF)

    recv(TOK_A)
    for t in range(N):
        x32[4 * t : 4 * t + 4, :] = tok_a[t].astype(F32)
    whole = x32[...].astype(BF)
    arranged = nn(whole, perm[...])
    for t in range(N):
        xs[t] = arranged[:, 64 * t : 64 * t + 64].astype(BF)
        xzs[t] = x32[:, 64 * t : 64 * t + 64].astype(BF)
    xt[y] = xs[y]
    xzt[z] = xzs[z]
    scatter(TOK_Y, "y", xs, xt)
    scatter(TOK_Z, "z", xzs, xzt)
    gather(W_UP, "y", gu, (2, 6, 1, 7))

    for phase in (G_MIX, G_MIZ, W_B, W_D):
        recv(phase)
    for t in range(N):
        gains[0:1, 32 * t : 32 * t + 32] = ggm[t]
        gains[1:2, 32 * t : 32 * t + 32] = ggz[t]
        bd[0:2, 32 * t : 32 * t + 32] = gb[t].astype(F32)
        bd[2:4, 32 * t : 32 * t + 32] = gd[t].astype(F32)
    eye64 = jnp.where(iota((SEQ, SEQ), 0) == iota((SEQ, SEQ), 1), 1.0, 0.0).astype(BF)
    recv(TOK_Y)
    token = nt(eye64, xt[...].reshape(256, SEQ))
    xf[...] = token
    squares = jnp.sum(token * token, axis=1, keepdims=True)
    normed = (token * gains[0:1, :]).astype(BF)
    aux = nt(normed, bd[...].astype(BF))
    lane = iota((SEQ, 128), 1)
    aux = jnp.where(lane == 4, squares, aux)
    high = aux.astype(BF).astype(F32)
    aux = jnp.where(lane < 64, high, pltpu.roll(aux - high, 64, 1))
    pys[:, :, 384:512] = aux.reshape(N, N, 128).astype(BF)
    recv(W_Y)
    pys[:, :, 0:384] = nn(normed, gy[...].reshape(256, 384)).reshape(N, N, 384).astype(BF)
    pyr[z] = pys[z]
    scatter(P_Y, "z", pys, pyr)
    recv(TOK_Z)
    other = (nt(eye64, xzt[...].reshape(256, SEQ)) * gains[1:2, :]).astype(BF)
    recv(W_Z)
    pzs[...] = nn(other, gz[...].reshape(256, 384)).reshape(N, N, 384).astype(BF)
    pzr[y] = pzs[y]
    scatter(P_Z, "y", pzs, pzr)
    recv(W_OUT)
    relay(W_OUT2, "y", go)
    r0 = iota((256, 256), 0)
    r1 = iota((256, 256), 1)
    turn = jnp.where((r0 == r1) & ((r0 // 4) % N == tp), 1.0, 0.0).astype(BF)

    def part(m):
        return jnp.where((i0 // (2 * m) == j0 // (2 * m)) & (i0 // m != j0 // m), tri[...], 0.0)

    def bmm(a, b):
        return lax.dot_general(a, b, (((2,), (1,)), ((0,), (0,))), preferred_element_type=F32, precision=HI)

    inverse = jnp.where(i0 == j0, 1.0, 0.0) - part(1)
    for m in (2, 4, 8, 16, 32):
        inverse = inverse - bmm(bmm(inverse, part(m)), inverse)
    tri[...] = inverse

    recv(W_UP)
    relay(W_UP2, "y", gu)
    gather(W_DOWN, "y", gdn, (2, 6, 1, 7))
    recv(P_Y)
    raw_y = jnp.sum(pyr[...].astype(F32), axis=0)
    aux = raw_y[:, 384:512]
    aux = aux + pltpu.roll(aux, 64, 1)
    row_scale = lax.rsqrt(aux[:, 4:5] / D + epsilon)
    raw_y = raw_y * row_scale
    recv(P_Z)
    raw_z = jnp.sum(pzr[...].astype(F32), axis=0) * row_scale
    both = range(2)
    tests, weights, invs = [], [], []
    for h in both:
        query = unit(silu(raw_y[:, 128 * h : 128 * h + 128]))
        key = unit(silu(raw_y[:, 256:384] if h == 0 else raw_z[:, 0:128]))
        weight = (1.0 / (1.0 + jnp.exp(-(aux[:, h : h + 1] * row_scale)))) * jnp.sum(key * query, axis=1, keepdims=True)
        tests.append(query - weight * key)
        weights.append(weight)
        invs.append(coef[N * h : N * h + N, :])
    scores = [rows_by(tests[h], kbuf[h], 2) * jnp.exp(totals[h] - gammas[h]) * invs[h] for h in both]
    solved = [
        own_row(bmm(jnp.broadcast_to(scores[h][None], (N, N, T_LEN)), tri[N * h : N * h + N])) * betas[h] for h in both
    ]
    taken = [rows_by(solved[h] * jnp.exp(gammas[h]) * invs[h], kbuf[h], 1) for h in both]
    moved = [jnp.exp(totals[h]) * tests[h] - taken[h] for h in both]
    from_state = [rows_by(moved[h], sbf[h], 1) for h in both]
    from_values = [rows_by(solved[h], vbuf[h], 1) for h in both]
    results = []
    for h in both:
        value = silu(raw_z[:, 128 + 128 * h : 256 + 128 * h])
        pre = aux[:, 2 + h : 3 + h] * row_scale
        soft = jnp.maximum(pre, 0.0) + jnp.log(1.0 + jnp.exp(-jnp.abs(pre)))
        fade = jnp.exp(-rate[h] * soft)
        results.append(fade * (from_state[h] + from_values[h]) + weights[h] * value)
    heads[z] = jnp.concatenate(results, axis=1).astype(BF)
    gather(HEADS, "z", heads)

    recv(W_OUT2)
    recv(G_MLP)
    for t in range(N):
        gains[2:3, 32 * t : 32 * t + 32] = ggl[t]
    recv(HEADS)
    gathered = heads[...].astype(F32).reshape(SEQ, 256).astype(BF)
    att[tp] = nt(gathered, go[...].reshape(256, 256)).astype(BF)
    gather(ATT, "tp", att)
    recv(W_UP2)
    recv(ATT)
    mixed[...] = (xf[...] + jnp.sum(att[...].astype(F32), axis=0)).astype(BF)
    mixer = mixed[...].astype(F32)
    normed = (mixer * gains[2:3, :]).astype(BF)
    ums[:, :, 0:1024] = nn(normed, gu[...].reshape(256, 1024)).reshape(N, N, 1024).astype(BF)
    squares = jnp.sum(mixer * mixer, axis=1, keepdims=True)
    high = squares.astype(BF).astype(F32)
    ums[:, :, 1024:1152] = jnp.where(lane < 64, high, squares - high).reshape(N, N, 128).astype(BF)
    umr[z] = ums[z]
    scatter(U_MAIN, "z", ums, umr)
    recv(W_DOWN)
    relay(W_DOWN2, "y", gdn)
    mixt[...] = nt(turn, mixed[...])
    recv(U_MAIN)
    raw = jnp.sum(umr[...].astype(F32), axis=0)
    row_scale = lax.rsqrt((raw[:, 1024:1025] + raw[:, 1088:1089]) / D + epsilon)
    raw = jnp.maximum(raw[:, 0:1024] * row_scale, 0.0)
    hid[z] = (raw * raw).astype(BF)
    gather(HID, "z", hid)
    recv(W_DOWN2)
    recv(HID)
    hidden = hid[...].astype(F32).reshape(SEQ, 1024).astype(BF)
    down_t[...] = nt(gdn[...].reshape(256, 1024), hidden) + mixt[...]
    for t in range(N * N):
        dns[t] = down_t[4 * t : 4 * t + 4, :].astype(BF)
    for a in (4, 3, 5, 2, 6, 1, 7, 0):
        for b in (4, 3, 5, 2, 6, 1, 7, 0):
            if a or b:
                to_y, to_tp = (y + a) % N, (tp + b) % N
                pltpu.make_async_remote_copy(
                    src_ref=dns.at[to_y * N + to_tp],
                    dst_ref=dnr.at[y * N + tp],
                    send_sem=send_sem.at[DOWN],
                    recv_sem=recv_sem.at[DOWN],
                    device_id=(z * N + to_y, to_tp),
                    device_id_type=MESH,
                ).start()
    dnr[y * N + tp] = dns[y * N + tp]
    for phase, buf, count in started:
        part_of = buf.at[pl.ds(0, count)]
        pltpu.make_async_copy(part_of, part_of, send_sem.at[phase]).wait()
    others = dnr.at[pl.ds(0, N * N - 1)]
    pltpu.make_async_copy(others, others, recv_sem.at[DOWN]).wait()
    for t in range(N):
        block = jnp.sum(dnr[N * t : N * t + N].astype(F32), axis=0)
        flat[0:4, 64 * t : 64 * t + 64] = block
    out[...] = nn(flat[...].astype(BF), perm[...])[0:4, :].astype(BF)
    pltpu.make_async_copy(others, others, send_sem.at[DOWN]).wait()


def local(
    tokens, mix_gain, query_weight, key_weight, value_weight, beta_weight, decay_weight, decay_rate, prior_state,
    tail_keys, tail_values, tail_beta, tail_decay, lengths, out_weight, mlp_gain, up_weight, down_weight,
):
    vmem = pl.BlockSpec(memory_space=pltpu.VMEM)
    hbm = pl.BlockSpec(memory_space=pl.ANY)
    specs = [hbm] * 18

    def v(*shape, dtype=BF):
        return pltpu.VMEM(shape, dtype)

    def f(*shape):
        return v(*shape, dtype=F32)

    result = pl.pallas_call(
        kernel,
        out_shape=jax.ShapeDtypeStruct((4, 512), BF),
        in_specs=specs,
        out_specs=vmem,
        scratch_shapes=[
            v(8, 4, 512), f(32, 512), v(512, 512), v(8, 32, 64), v(8, 32, 64), v(8, 32, 64), v(8, 32, 64), f(64, 256),
            v(8, 32, 384), v(8, 32, 384), v(8, 2, 32), v(8, 2, 32), f(8, 1, 32), f(8, 1, 32), f(8, 1, 32),
            v(8, 32, 256), v(8, 32, 1024), v(8, 32, 1024), f(128, 256), f(8, 256),
            v(2, 8, 64, 128), v(2, 8, 64, 128), f(2, 8, 128, 128), v(2, 8, 128, 128), f(8, 2, 64), f(8, 2, 64),
            f(16, 64, 64), f(16, 64),
            v(8, 8, 512), v(8, 8, 512), v(8, 8, 384), v(8, 8, 384),
            v(8, 8, 256), v(8, 64, 256), v(64, 256), f(256, 64),
            v(8, 8, 1152), v(8, 8, 1152),
            v(8, 8, 1024), f(256, 64), v(64, 4, 64), v(64, 4, 64), f(8, 512),
            pltpu.SMEM((8,), jnp.int32), pltpu.SMEM((2,), F32),
            pltpu.SemaphoreType.DMA((23,)), pltpu.SemaphoreType.DMA((23,)), pltpu.SemaphoreType.DMA((23,)),
        ],
        compiler_params=pltpu.CompilerParams(collective_id=0, has_side_effects=True),
    )(
        tokens.T, mix_gain.reshape(1, -1), query_weight, key_weight, value_weight, beta_weight.T, decay_weight.T,
        decay_rate, prior_state, tail_keys, tail_values, tail_beta, tail_decay, lengths, out_weight.T,
        mlp_gain.reshape(1, -1), up_weight, down_weight.T,
    )
    return result.T


def solution(mesh):
    kt = ("kv", "tp")
    return jax.shard_map(
        local,
        mesh=mesh,
        in_specs=(
            P(None, kt), P("kv"), P("kv", "tp"), P("kv", "tp"), P("kv", "tp"), P("kv", "tp"), P("kv", "tp"), P("tp"),
            P("kv", "tp", None, None), P("kv", "tp", None, None), P("kv", "tp", None, None),
            P("kv", "tp", None), P("kv", "tp", None), P("kv"), P("tp", "kv"), P("kv"), P("kv", "tp"), P("tp", "kv"),
        ),
        out_specs=P(None, kt),
        check_vma=False,
    )
```
